32 devices in a mesh: grp: 2 (over x), ep: 16 (over z, y, core).
Axes of the slice: x: 2, y: 2, z: 4, core: 2. Of those that a mesh axis runs over, the one named last changes fastest.
Arguments:
- tokens: bfloat16 [128, 2048], P(('grp', 'ep')), parts along dimension 0, may hold values from -6 to 6
- memory_state: float32 [128, 4, 256, 512], P(('grp', 'ep')), parts along dimension 0, may hold values from -0.6 to 0.6
- max_state: float32 [128, 4], P(('grp', 'ep')), parts along dimension 0, may hold values from -4 to 4
- norm_gain: float32 [2048], replicated, may hold values from 0.1 to 1.9
- query_weight: bfloat16 [2048, 1024], P(None, 'ep'), may hold values from -0.125 to 0.125
- key_weight: bfloat16 [2048, 1024], P(None, 'ep'), may hold values from -0.125 to 0.125
- value_weight: bfloat16 [2048, 2048], P(None, 'ep'), may hold values from -0.125 to 0.125
- output_gate: bfloat16 [2048, 2048], P(None, 'ep'), may hold values from -0.125 to 0.125
- input_gate: bfloat16 [2048, 4], replicated, may hold values from -0.125 to 0.125
- forget_gate: bfloat16 [2048, 4], replicated, may hold values from -0.125 to 0.125
- forget_bias: float32 [4], replicated, may hold values from -2 to 4
- head_gain: float32 [2048], replicated, may hold values from 0.1 to 1.9
- output_weight: bfloat16 [2048, 2048], P(None, 'ep'), may hold values from -0.125 to 0.125
- expert_norm: float32 [2048], replicated, may hold values from 0.1 to 1.9
- routed_experts: int32 [128, 4], P(('grp', 'ep')), parts along dimension 0, may hold values from 0 to 15, as said below
- route_weights: float32 [128, 4], P(('grp', 'ep')), parts along dimension 0, may hold values from 0.1 to 1
- expert_gate: bfloat16 [16, 2048, 512], P('ep'), may hold values from -0.125 to 0.125
- expert_lift: bfloat16 [16, 2048, 512], P('ep'), may hold values from -0.125 to 0.125
- expert_down: bfloat16 [16, 512, 2048], P('ep'), may hold values from -0.25 to 0.25
Outputs:
- layer_out: bfloat16 [128, 2048], P(('grp', 'ep')), parts along dimension 0
- new_memory: float32 [128, 4, 256, 512], P(('grp', 'ep')), parts along dimension 0
- new_max: float32 [128, 4], P(('grp', 'ep')), parts along dimension 0
The draws below stay inside these ranges and needn't reach their ends.
There are 2 independent parts, one for each index of `grp`. The reference program is written for one: setup_inputs(seed, part) draws one part's arguments, and reference() takes and returns one part's arrays. A program takes and returns all parts, laid end to end along the dimension named above; an argument that names none is the same for every part. Nothing has to cross between parts.
Inputs may be any that keep to these rules, and one draw needn't show every extreme that they name: `routed_experts`: each row names 4 different experts of one group (expert e lies in group e // 4). No expert is named by more than 2 rows of one device, and some device has an expert named by 2 of its rows.
All inputs are finite; a program needn't handle non-finite values.
Results may differ from the reference program's by a relative error of at most 0.013.
Values may be sent and summed in bfloat16 or wider, within the bound.
A program may use at most 64 MiB of HBM per device.

```python
import math
import jax
import jax.numpy as jnp
from jax import lax

D = 2048
HEADS = 4
DQK = 256
DV = 512
DE = 512
TOP = 4
GROUPS = 4
EXPERTS = 16
EPG = 4
SEQ_DEV = 4
SEQS = 64


def draw_routed_experts(key, part):
    base = jax.random.fold_in(key, 11)
    keys_all = jax.random.split(base, 4)
    device_count = SEQS // SEQ_DEV
    order = jax.random.permutation(keys_all[0], GROUPS)
    lowest = jnp.minimum(jax.random.randint(keys_all[1], (device_count,), 0, GROUPS), jax.random.randint(keys_all[2], (device_count,), 0, GROUPS))
    device_group = order[lowest]
    scores = jax.random.randint(keys_all[3], (device_count, EPG), 0, 1 << 20) * EPG + jnp.arange(EPG, dtype=jnp.int32)[None, :]
    shuffled = jnp.argsort(scores, axis=1).astype(jnp.int32)
    row_index = jnp.arange(SEQS, dtype=jnp.int32)
    device_of = row_index // SEQ_DEV
    pair_index = row_index % SEQ_DEV // 2
    halves = EPG // TOP
    slot_index = pair_index % (GROUPS * halves)
    group_ids = (device_group[device_of] + slot_index // halves) % GROUPS
    half_ids = slot_index % halves
    positions = half_ids[:, None] * TOP + jnp.arange(TOP, dtype=jnp.int32)[None, :]
    within = jnp.take_along_axis(shuffled[device_of], positions, axis=1)
    chosen = group_ids[:, None] * EPG + within
    return chosen.astype(jnp.int32)


def block_levels(key, dims, cuts, smallest, top_value):
    level, own = 1.0, jax.random.fold_in(key, 6)
    for dim, blocks in cuts:
        heights = jnp.exp(jax.random.uniform(jax.random.fold_in(own, dim), (blocks,), jnp.float32, smallest / len(cuts), top_value / len(cuts)))
        level = level * jnp.repeat(heights, dims[dim] // blocks).reshape([-1 if axis == dim else 1 for axis in range(len(dims))])
    return level


def noise(stream_key, dims, width, most, cuts=(), held_as=jnp.bfloat16):
    values = width * jax.random.normal(stream_key, dims, jnp.float32)
    if cuts:
        values = values * block_levels(stream_key, dims, cuts, -0.22, 0.18)
    return jnp.clip(values, -most, most).astype(held_as)


def setup_inputs(seed: int = 0, part: int = 0) -> dict:
    arg_keys = jax.random.split(jax.random.key(seed), 20)
    part_splits = jax.random.split(jax.random.fold_in(arg_keys[19], part), 20)
    tokens = noise(part_splits[0], (SEQS, D), 1.0, 6.0, ((0, 16),))
    memory_state = noise(part_splits[1], (SEQS, HEADS, DQK, DV), 0.1, 0.6, ((0, 16),), jnp.float32)
    max_state = noise(part_splits[2], (SEQS, HEADS), 1.0, 4.0, ((0, 16),), jnp.float32)
    norm_gain = jnp.clip(1.0 + 0.18 * jax.random.normal(arg_keys[3], (D,), jnp.float32), 0.1, 1.9)
    query_weight = noise(arg_keys[4], (D, HEADS * DQK), D ** -0.5, 0.125, ((1, 16),))
    key_weight = noise(arg_keys[5], (D, HEADS * DQK), D ** -0.5, 0.125, ((1, 16),))
    value_weight = noise(arg_keys[6], (D, HEADS * DV), D ** -0.5, 0.125, ((1, 16),))
    output_gate = noise(arg_keys[7], (D, HEADS * DV), D ** -0.5, 0.125, ((1, 16),))
    input_gate = noise(arg_keys[8], (D, HEADS), D ** -0.5, 0.125)
    forget_gate = noise(arg_keys[9], (D, HEADS), D ** -0.5, 0.125)
    forget_bias = jnp.clip(jax.random.uniform(arg_keys[10], (HEADS,), jnp.float32, -2.0, 4.0), -2.0, 4.0)
    head_gain = jnp.clip(1.0 + 0.18 * jax.random.normal(arg_keys[11], (HEADS * DV,), jnp.float32), 0.1, 1.9)
    output_weight = noise(arg_keys[12], (HEADS * DV, D), (HEADS * DV) ** -0.5, 0.125, ((1, 16),))
    expert_norm = jnp.clip(1.0 + 0.18 * jax.random.normal(arg_keys[13], (D,), jnp.float32), 0.1, 1.9)
    routed_experts = draw_routed_experts(jax.random.fold_in(jax.random.fold_in(arg_keys[19], part), 71), part)
    route_weights = jnp.clip(jnp.exp(math.log(1.0) - 2.3025851 * jax.random.uniform(part_splits[15], (SEQS, TOP), jnp.float32) ** block_levels(part_splits[15], (SEQS, TOP), ((0, 16),), -0.2, 0.2)), 0.1, 1.0)
    expert_gate = noise(arg_keys[16], (EXPERTS, D, DE), D ** -0.5, 0.125, ((0, 16),))
    expert_lift = noise(arg_keys[17], (EXPERTS, D, DE), D ** -0.5, 0.125, ((0, 16),))
    expert_down = noise(arg_keys[18], (EXPERTS, DE, D), DE ** -0.5, 0.25, ((0, 16),))
    return {"tokens": tokens, "memory_state": memory_state, "max_state": max_state, "norm_gain": norm_gain, "query_weight": query_weight, "key_weight": key_weight, "value_weight": value_weight, "output_gate": output_gate, "input_gate": input_gate, "forget_gate": forget_gate, "forget_bias": forget_bias, "head_gain": head_gain, "output_weight": output_weight, "expert_norm": expert_norm, "routed_experts": routed_experts, "route_weights": route_weights, "expert_gate": expert_gate, "expert_lift": expert_lift, "expert_down": expert_down}


epsilon = 1e-06

def scaled_norm(entries, gain):
    return entries * lax.rsqrt(lax.optimization_barrier(jnp.mean(entries * entries, axis=-1, keepdims=True)) + epsilon) * gain

def reference(tokens, memory_state, max_state, norm_gain, query_weight, key_weight, value_weight, output_gate, input_gate, forget_gate, forget_bias, head_gain, output_weight, expert_norm, routed_experts, route_weights, expert_gate, expert_lift, expert_down):
    seq_count = tokens.shape[0]
    inputs = tokens.astype(jnp.float32)
    normed = scaled_norm(inputs, norm_gain).astype(jnp.bfloat16)
    queries = jnp.dot(normed, query_weight, preferred_element_type=jnp.float32).astype(jnp.bfloat16)
    keys_proj = jnp.dot(normed, key_weight, preferred_element_type=jnp.float32).astype(jnp.bfloat16)
    values_proj = jnp.dot(normed, value_weight, preferred_element_type=jnp.float32).astype(jnp.bfloat16)
    gates = jnp.dot(normed, output_gate, preferred_element_type=jnp.float32).astype(jnp.bfloat16)
    input_logit = jnp.dot(normed, input_gate, preferred_element_type=jnp.float32)
    log_forget = jax.nn.log_sigmoid(jnp.dot(normed, forget_gate, preferred_element_type=jnp.float32) + forget_bias)
    query_heads = queries.astype(jnp.float32).reshape(seq_count, HEADS, DQK)
    key_heads = keys_proj.astype(jnp.float32).reshape(seq_count, HEADS, DQK) * DQK ** (-0.5)
    value_heads = values_proj.astype(jnp.float32).reshape(seq_count, HEADS, DV)
    new_max = jnp.maximum(log_forget + max_state, input_logit)
    carried = jnp.exp(log_forget + max_state - new_max)
    written = jnp.exp(input_logit - new_max)
    new_memory = carried[:, :, None, None] * memory_state + (written[:, :, None] * key_heads)[:, :, :, None] * value_heads[:, :, None, :]
    readout = jnp.einsum('shd,shde->she', query_heads, new_memory, precision=lax.Precision.HIGHEST)
    gate_heads = jax.nn.sigmoid(gates.astype(jnp.float32).reshape(seq_count, HEADS, DV))
    mixed = (scaled_norm(readout, head_gain.reshape(HEADS, DV)) * gate_heads).reshape(seq_count, HEADS * DV).astype(jnp.bfloat16)
    branch = jnp.dot(mixed, output_weight, preferred_element_type=jnp.float32).astype(jnp.bfloat16)
    residual = (inputs + branch.astype(jnp.float32)).astype(jnp.bfloat16)
    expert_in = scaled_norm(residual.astype(jnp.float32), expert_norm).astype(jnp.bfloat16)

    def one_token(packed):
        token_row, picked_experts, weights = packed
        token_float = token_row.astype(jnp.float32)
        gate_value = jnp.einsum('d,kdf->kf', token_float, expert_gate[picked_experts].astype(jnp.float32))
        lift_value = jnp.einsum('d,kdf->kf', token_float, expert_lift[picked_experts].astype(jnp.float32))
        hidden = (jax.nn.silu(gate_value) * lift_value).astype(jnp.bfloat16)
        expert_rows = jnp.einsum('kf,kfd->kd', hidden.astype(jnp.float32), expert_down[picked_experts].astype(jnp.float32)).astype(jnp.bfloat16)
        weighted = lax.optimization_barrier((weights[:, None] * expert_rows.astype(jnp.float32)).astype(jnp.bfloat16))
        return lax.optimization_barrier(jnp.sum(weighted.astype(jnp.float32), axis=0))
    expert_sum = lax.map(one_token, (expert_in, routed_experts, route_weights))
    layer_out = (residual.astype(jnp.float32) + expert_sum).astype(jnp.bfloat16)
    return (layer_out, new_memory, new_max)
```

```python
import functools

import jax
import jax.numpy as jnp
from jax import lax
from jax.experimental import pallas as pl
from jax.experimental.pallas import tpu as pltpu
from jax.sharding import PartitionSpec as P

epsilon = 1e-06
F32 = jnp.float32
BF16 = jnp.bfloat16
ANY = pl.BlockSpec(memory_space=pl.ANY)
HBM = pl.BlockSpec(memory_space=pltpu.HBM)
VMEM = pl.BlockSpec(memory_space=pltpu.VMEM)
SLOTS = 2


def scaled_norm(entries, gain):
    return entries * lax.rsqrt(jnp.mean(entries * entries, axis=-1, keepdims=True) + epsilon) * gain


def flip(me, mask):
    peer, bit = me, 1
    while bit <= mask:
        if mask & bit:
            peer = peer + bit * (1 - 2 * lax.rem(lax.div(me, bit), 2))
        bit *= 2
    return peer


def remote(source, target, sems, phase, slot, peer):
    send_sem, recv_sem = sems
    return pltpu.make_async_remote_copy(
        src_ref=source,
        dst_ref=target,
        send_sem=send_sem.at[phase, slot],
        recv_sem=recv_sem.at[phase, slot],
        device_id={"ep": peer},
    )


def exchange(n, me, source, landing, sems, phase):
    copies = []
    for mask in range(n - 1, 0, -1):
        peer = flip(me, mask)
        copies.append(remote(source(peer), landing.at[me], sems, phase, mask, peer))
        copies[-1].start()
    return copies


def gather(n, me, source, landing, sems, phase):
    partner = flip(me, 1)
    far = {m: remote(source, landing.at[me], sems, phase, m, flip(me, m)) for m in range(n - 2, 0, -2)}
    for piece in far.values():
        piece.start()
    near = [remote(source, landing.at[me], sems, phase, 1, partner)]
    near[0].start()

    def relay():
        for m in range(2, n, 2):
            far[m].wait_recv()
            origin = flip(me, m)
            near.append(remote(landing.at[origin], landing.at[origin], sems, phase, m + 1, partner))
            near[-1].start()
        finish(near)
        return list(far.values()) + near

    return relay


def finish(copies):
    for copy in copies:
        copy.wait_recv()


def drain(copies):
    for copy in copies:
        copy.wait_send()


def tall(table):
    return table if table.shape[1] % 128 == 0 else table.T


def across(lhs, table):
    return lax.dot_general(lhs, table, (((1,), (1,)), ((), ())), preferred_element_type=F32)


def apply(lhs, table, columns):
    if columns % 128 == 0:
        return jnp.dot(lhs, table, preferred_element_type=F32)
    return across(lhs, table)


def rows_of(ref, n, start, size):
    return jnp.concatenate([ref[j, :, start : start + size].astype(F32) for j in range(n)], axis=0)


def own_columns(ref, n, me, columns):
    if columns % 128 == 0:
        at = pl.ds(pl.multiple_of(me * columns, 128), columns)
        return jnp.concatenate([ref[j, :, at].astype(F32) for j in range(n)], axis=0)
    share = 128 // columns
    at = pl.ds(pl.multiple_of(lax.div(me, share) * 128, 128), 128)
    wide = jnp.concatenate([ref[j, :, at].astype(F32) for j in range(n)], axis=0)
    part = lax.rem(me, share)
    picked = wide[:, :columns]
    for i in range(1, share):
        picked = jnp.where(part == i, wide[:, i * columns : (i + 1) * columns], picked)
    return picked


def layer_kernel(
    n, heads, key_size, value_size, names_width,
    tokens, memory, max_state, norm_gain, wv, wg, wq, wk, w_in, w_forget, forget_bias,
    head_gain, wo, expert_norm, routed, route_weights, w_gate, w_lift, w_down,
    new_memory, results, residual_out, picks_out, max_out,
    tok_s, max_s, ngain_s, v_w, g_w, q_w, k_w, in_w, forget_w, bias_s,
    hgain_s, o_w, egain_s, routed_s, rw_s, gate_w, lift_w, down_w,
    all_s, names_s, pick_s, x_s, proj_s, back_s, qt_s, kt_s, v_s, c_s, ro_s, mix_s,
    res_s, needed_s, own_s, owned_s, out_s,
    local_sem, mem_sem, send_sem, recv_sem,
):
    me = lax.axis_index("ep")
    barrier = pltpu.get_barrier_semaphore()
    for mask in range(n - 1, 0, -1):
        pl.semaphore_signal(barrier, inc=1, device_id={"ep": flip(me, mask)})
    rows, width = tokens.shape
    sems = (send_sem, recv_sem)
    pairs = [
        (tokens, tok_s.at[:, pl.ds(0, width)]), (routed, routed_s), (norm_gain, ngain_s),
        (w_in, in_w), (w_forget, forget_w), (forget_bias, bias_s), (max_state, max_s),
        (route_weights, rw_s), (wv, v_w), (wg, g_w), (wq, q_w), (wk, k_w),
        (head_gain, hgain_s), (expert_norm, egain_s), (wo, o_w),
        (w_gate.at[0], gate_w), (w_lift.at[0], lift_w), (w_down.at[0], down_w),
    ]
    loads = [pltpu.make_async_copy(a, b, local_sem.at[i]) for i, (a, b) in enumerate(pairs)]
    for load in loads[:12]:
        load.start()

    def fetch(h, s):
        return pltpu.make_async_copy(memory.at[s, h], new_memory.at[s, h], mem_sem.at[h, s])

    for h in range(heads):
        for s in range(rows):
            fetch(h, s).start()
    for load in loads[12:]:
        load.start()

    for load in loads[:8]:
        load.wait()
    lane = lax.broadcasted_iota(jnp.int32, (rows, names_width), 1)
    which = routed_s[...]
    weights = rw_s[...]
    taken = jnp.zeros((1, names_width), F32)
    chosen = []
    named = jnp.zeros((rows, names_width), F32)
    weighed = jnp.zeros((rows, names_width), F32)
    for slot in range(SLOTS):
        for k in range(which.shape[1]):
            hit = lane == which[:, k : k + 1] + slot * n
            named = named + hit.astype(F32)
            weighed = weighed + jnp.where(hit, weights[:, k : k + 1], 0.0)
    slot_of = (lax.broadcasted_iota(jnp.int32, (1, names_width), 1) >= n).astype(F32)
    for r in range(rows):
        chosen.append(named[r : r + 1] * (taken == slot_of).astype(F32))
        taken = taken + named[r : r + 1]
    chosen = jnp.concatenate(chosen, axis=0)
    tok_s[:, width:] = chosen.astype(BF16)
    picks_out[...] = chosen * weighed

    gain = ngain_s[...]
    own = scaled_norm(tok_s[:, :width].astype(F32), gain).astype(BF16)
    input_logit = across(own, in_w[...])
    raw = across(own, forget_w[...]) + bias_s[...]
    log_forget = jnp.minimum(raw, 0.0) - jnp.log1p(jnp.exp(-jnp.abs(raw)))
    prior = log_forget + max_s[...]
    new_max = jnp.maximum(prior, input_logit)
    max_out[...] = new_max
    carried = jnp.exp(prior - new_max)
    written = jnp.exp(input_logit - new_max) * key_size**-0.5

    pl.semaphore_wait(barrier, n - 1)
    relay = gather(n, me, tok_s, all_s, sems, 0)
    all_s[me] = tok_s[...]
    for load in loads[8:12]:
        load.wait()
    sent = relay()
    normed = scaled_norm(rows_of(all_s, n, 0, width), gain).astype(BF16)
    cq, cv = heads * key_size // n, heads * value_size // n
    tables = [v_w[...], g_w[...], q_w[...], k_w[...]]
    projected = jnp.concatenate(
        [apply(normed, table, c) for table, c in zip(tables, (cv, cv, cq, cq))], axis=1
    )
    for j in range(n):
        proj_s[j] = projected[j * rows : (j + 1) * rows].astype(BF16)
    back = exchange(n, me, lambda peer: proj_s.at[peer], back_s, sems, 1)
    back_s[me] = proj_s[me]

    columns = res_s.shape[1]
    x_s[...] = own_columns(all_s, n, me, columns)
    names_s[...] = rows_of(all_s, n, width, names_width).T
    wanted = SLOTS * n
    place = lax.broadcasted_iota(jnp.int32, (wanted, n * rows), 0)
    row = lax.broadcasted_iota(jnp.int32, (wanted, n * rows), 1)
    first = (place - place % SLOTS) // SLOTS * rows
    inside = (row >= first) & (row < first + rows)
    even = place % SLOTS == 0
    for j in range(n):
        value = jnp.where(even, names_s[j : j + 1, :], names_s[n + j : n + j + 1, :])
        pick_s[j] = jnp.where(inside, value, 0.0).astype(BF16)
    loads[12].wait()
    loads[13].wait()
    loads[14].wait()
    for h in range(heads):
        for s in range(rows):
            fetch(h, s).wait()
    finish(back)

    pieces = [back_s[j].astype(F32) for j in range(n)]
    v = jnp.concatenate([b[:, :cv] for b in pieces], axis=1)
    g = jnp.concatenate([b[:, cv : 2 * cv] for b in pieces], axis=1)
    q = jnp.concatenate([b[:, 2 * cv : 2 * cv + cq] for b in pieces], axis=1)
    k = jnp.concatenate([b[:, 2 * cv + cq :] for b in pieces], axis=1)
    pad = jnp.zeros((-rows % 8, q.shape[1]), F32)
    qt_s[...] = jnp.concatenate([q, pad], axis=0).T
    kt_s[...] = jnp.concatenate([k, pad], axis=0).T
    for h in range(heads):
        c_s[h] = jnp.broadcast_to(carried[:, h : h + 1], (rows, value_size))
        v_s[h] = v[:, h * value_size : (h + 1) * value_size] * written[:, h : h + 1]
    step = 32

    def read(h, carry):
        for s in range(rows):

            def chunk(r, total):
                at = pl.multiple_of(r * step, step)
                col = pl.ds(pl.multiple_of(h * key_size + at, step), step)
                terms = qt_s[col, s : s + 1] * new_memory[s, h, pl.ds(at, step), :]
                return total + jnp.sum(terms.reshape(step // 8, 8, value_size), axis=0)

            total = lax.fori_loop(
                0, key_size // step, chunk, jnp.zeros((8, value_size), F32), unroll=True
            )
            ro_s[h, s : s + 1, :] = jnp.sum(total, axis=0, keepdims=True)
        return carry

    lax.fori_loop(0, heads, read, 0)
    for h in range(heads):
        cols = slice(h * value_size, (h + 1) * value_size)
        keys = slice(h * key_size, (h + 1) * key_size)
        match = jnp.sum(q[:, keys] * k[:, keys], axis=1, keepdims=True)
        readout = c_s[h] * ro_s[h] + match * v_s[h]
        part = scaled_norm(readout, hgain_s[:, cols]) * jax.nn.sigmoid(g[:, cols])
        mix_s[me, :, cols] = part.astype(BF16)
    relay = gather(n, me, mix_s.at[me], mix_s, sems, 2)

    def update(h, carry):
        for s in range(rows):
            keep = c_s[h, s : s + 1, :]
            values = v_s[h, s : s + 1, :]

            def chunk(r, nothing):
                at = pl.multiple_of(r * step, step)
                col = pl.ds(pl.multiple_of(h * key_size + at, step), step)
                new_memory[s, h, pl.ds(at, step), :] = (
                    keep * new_memory[s, h, pl.ds(at, step), :] + kt_s[col, s : s + 1] * values
                )
                return nothing

            lax.fori_loop(0, key_size // step, chunk, 0, unroll=True)
        return carry

    lax.fori_loop(0, heads, update, 0)
    sent += relay()
    branch = apply(rows_of(mix_s, n, 0, width).astype(BF16), o_w[...], columns).astype(BF16)
    residual = (x_s[...] + branch.astype(F32)).astype(BF16)
    picked = jnp.dot(
        pick_s[...].reshape(n * wanted, n * rows), residual, preferred_element_type=F32
    ).astype(BF16)
    res_s[...] = picked
    there = exchange(
        n, me, lambda peer: res_s.at[pl.ds(pl.multiple_of(peer * wanted, wanted), wanted)],
        needed_s, sems, 3,
    )
    needed_s[me] = res_s[pl.ds(pl.multiple_of(me * wanted, wanted), wanted)]
    whole = residual.astype(F32)
    for j in range(n):
        own_s[j] = whole[j * rows : (j + 1) * rows].astype(BF16)
    home = exchange(n, me, lambda peer: own_s.at[peer], owned_s, sems, 4)
    owned_s[me] = own_s[me]
    for load in loads[15:]:
        load.wait()
    finish(there)
    needed = jnp.concatenate([needed_s[j].astype(F32) for j in range(n)], axis=1)
    expert_in = scaled_norm(needed, egain_s[...]).astype(BF16)
    gate_value = jnp.dot(expert_in, gate_w[...], preferred_element_type=F32)
    lift_value = jnp.dot(expert_in, lift_w[...], preferred_element_type=F32)
    hidden = (jax.nn.silu(gate_value) * lift_value).astype(BF16)
    result = jnp.dot(hidden, down_w[...], preferred_element_type=F32)
    for j in range(n):
        out_s[j] = result[j * SLOTS : (j + 1) * SLOTS].astype(BF16)
    last = exchange(n, me, lambda peer: out_s.at[peer], results, sems, 5)
    results[me] = out_s[me]
    finish(home)
    residual_out[...] = jnp.concatenate([owned_s[j].astype(F32) for j in range(n)], axis=1)
    drain(sent + back + there + home)
    finish(last)
    drain(last)


def combine_kernel(
    memory, results, residual, picks, new_max_in,
    layer_out, new_memory, max_out,
    out_s, top_s, mem_sem, sem,
):
    n, slots, width = results.shape
    rows, heads = new_max_in.shape

    def save(h, s):
        return pltpu.make_async_copy(memory.at[s, h], new_memory.at[s, h], mem_sem.at[h, s])

    for h in range(heads):
        for s in range(rows):
            save(h, s).start()
    top_s[...] = new_max_in[...]
    top = pltpu.make_async_copy(top_s, max_out, sem.at[0])
    top.start()
    weights = picks[...]
    total = jnp.zeros((rows, width), F32)
    for j in range(n):
        block = results[j].astype(F32)
        for s in range(slots):
            weight = weights[:, s * n + j : s * n + j + 1]
            total = total + (weight * block[s : s + 1]).astype(BF16).astype(F32)
    out_s[...] = (residual[...] + total).astype(BF16)
    out = pltpu.make_async_copy(out_s, layer_out, sem.at[1])
    out.start()
    for h in range(heads):
        for s in range(rows):
            save(h, s).wait()
    top.wait()
    out.wait()


def body(
    tokens, memory_state, max_state, norm_gain, query_weight, key_weight, value_weight,
    output_gate, input_gate, forget_gate, forget_bias, head_gain, output_weight, expert_norm,
    routed_experts, route_weights, expert_gate, expert_lift, expert_down,
):
    n = lax.axis_size("ep")
    rows, width = tokens.shape
    _, heads, key_size, value_size = memory_state.shape
    hidden = expert_gate.shape[2]
    cq, cv, columns = query_weight.shape[1], value_weight.shape[1], output_weight.shape[1]
    total_cols = 2 * cq + 2 * cv
    wv, wg, wq, wk = (tall(t) for t in (value_weight, output_gate, query_weight, key_weight))
    wo = tall(output_weight)
    names_width = -(-SLOTS * n // 128) * 128
    wanted = SLOTS * n
    sds = jax.ShapeDtypeStruct
    small = sds((rows, heads), F32)
    padded = -(-rows // 8) * 8
    new_memory, results, residual, picks, new_max = pl.pallas_call(
        functools.partial(layer_kernel, n, heads, key_size, value_size, names_width),
        out_shape=(
            pltpu.VMEM(memory_state.shape, F32),
            pltpu.VMEM((n, SLOTS, width), BF16),
            pltpu.VMEM((rows, width), F32),
            pltpu.VMEM((rows, names_width), F32),
            pltpu.VMEM((rows, heads), F32),
        ),
        in_specs=[HBM] * 19,
        out_specs=[VMEM] * 5,
        scratch_shapes=[
            pltpu.VMEM((rows, width + names_width), BF16),
            pltpu.VMEM((rows, heads), F32),
            pltpu.VMEM((1, width), F32),
            pltpu.VMEM(wv.shape, BF16),
            pltpu.VMEM(wg.shape, BF16),
            pltpu.VMEM(wq.shape, BF16),
            pltpu.VMEM(wk.shape, BF16),
            pltpu.VMEM((heads, width), BF16),
            pltpu.VMEM((heads, width), BF16),
            pltpu.VMEM((1, heads), F32),
            pltpu.VMEM((1, width), F32),
            pltpu.VMEM(wo.shape, BF16),
            pltpu.VMEM((1, width), F32),
            pltpu.VMEM(routed_experts.shape, jnp.int32),
            pltpu.VMEM(route_weights.shape, F32),
            pltpu.VMEM((width, hidden), BF16),
            pltpu.VMEM((width, hidden), BF16),
            pltpu.VMEM((hidden, width), BF16),
            pltpu.VMEM((n, rows, width + names_width), BF16),
            pltpu.VMEM((names_width, n * rows), F32),
            pltpu.VMEM((n, wanted, n * rows), BF16),
            pltpu.VMEM((n * rows, columns), F32),
            pltpu.VMEM((n, rows, total_cols), BF16),
            pltpu.VMEM((n, rows, total_cols), BF16),
            pltpu.VMEM((heads * key_size, padded), F32),
            pltpu.VMEM((heads * key_size, padded), F32),
            pltpu.VMEM((heads, rows, value_size), F32),
            pltpu.VMEM((heads, rows, value_size), F32),
            pltpu.VMEM((heads, rows, value_size), F32),
            pltpu.VMEM((n, rows, width), BF16),
            pltpu.VMEM((n * wanted, columns), BF16),
            pltpu.VMEM((n, wanted, columns), BF16),
            pltpu.VMEM((n, rows, columns), BF16),
            pltpu.VMEM((n, rows, columns), BF16),
            pltpu.VMEM((n, SLOTS, width), BF16),
            pltpu.SemaphoreType.DMA((18,)),
            pltpu.SemaphoreType.DMA((heads, rows)),
            pltpu.SemaphoreType.DMA((6, n)),
            pltpu.SemaphoreType.DMA((6, n)),
        ],
        compiler_params=pltpu.CompilerParams(
            collective_id=0, has_side_effects=True, vmem_limit_bytes=40 << 20
        ),
        name="layer",
    )(*(
        pltpu.with_memory_space_constraint(x, pltpu.HBM)
        for x in (
            tokens, memory_state, max_state, norm_gain.reshape(1, -1), wv, wg, wq, wk,
            input_gate.T, forget_gate.T, forget_bias.reshape(1, -1), head_gain.reshape(1, -1), wo,
            expert_norm.reshape(1, -1), routed_experts, route_weights,
            expert_gate, expert_lift, expert_down,
        )
    ))
    layer_out, new_memory, new_max = pl.pallas_call(
        combine_kernel,
        out_shape=(sds((rows, width), BF16), sds(memory_state.shape, F32), small),
        in_specs=[VMEM] * 5,
        out_specs=[ANY] * 3,
        scratch_shapes=[
            pltpu.VMEM((rows, width), BF16),
            pltpu.VMEM((rows, heads), F32),
            pltpu.SemaphoreType.DMA((heads, rows)),
            pltpu.SemaphoreType.DMA((2,)),
        ],
        compiler_params=pltpu.CompilerParams(vmem_limit_bytes=8 << 20),
        name="combine",
    )(new_memory, results, residual, picks, new_max)
    return layer_out, new_memory, new_max


def solution(mesh):
    both = ("grp", "ep")
    return jax.shard_map(
        body,
        mesh=mesh,
        in_specs=(
            P(both, None), P(both, None, None, None), P(both, None), P(),
            P(None, "ep"), P(None, "ep"), P(None, "ep"), P(None, "ep"),
            P(), P(), P(), P(), P(None, "ep"), P(),
            P(both, None), P(both, None),
            P("ep", None, None), P("ep", None, None), P("ep", None, None),
        ),
        out_specs=(P(both, None), P(both, None, None, None), P(both, None)),
        check_vma=False,
    )
```

```python
import functools

import jax
import jax.numpy as jnp
from jax import lax
from jax.experimental import pallas as pl
from jax.experimental.pallas import tpu as pltpu
from jax.sharding import PartitionSpec as P

epsilon = 1e-06
F32 = jnp.float32
BF16 = jnp.bfloat16
ANY = pl.BlockSpec(memory_space=pl.ANY)
HBM = pl.BlockSpec(memory_space=pltpu.HBM)
VMEM = pl.BlockSpec(memory_space=pltpu.VMEM)
SLOTS = 2


def scaled_norm(entries, gain):
    return entries * lax.rsqrt(jnp.mean(entries * entries, axis=-1, keepdims=True) + epsilon) * gain


def flip(me, mask):
    peer, bit = me, 1
    while bit <= mask:
        if mask & bit:
            peer = peer + bit * (1 - 2 * lax.rem(lax.div(me, bit), 2))
        bit *= 2
    return peer


def remote(source, target, send_sem, recv_sem, peer):
    return pltpu.make_async_remote_copy(
        src_ref=source, dst_ref=target, send_sem=send_sem, recv_sem=recv_sem, device_id={"ep": peer}
    )


def exchange(n, me, source, landing, send_sem, recv_sem):
    for mask in range(n - 1, 0, -1):
        peer = flip(me, mask)
        remote(source(peer), landing.at[me], send_sem, recv_sem(mask), peer).start()


def spread(n, me, source, target, send_sem, far_sem, near_sem):
    for mask in [*range(n - 2, 0, -2), 1]:
        sem = near_sem if mask == 1 else far_sem.at[mask // 2]
        remote(source, target, send_sem, sem, flip(me, mask)).start()


def relay(n, me, block_of, send_sem, far_sem, near_sem):
    partner = flip(me, 1)
    for mask in range(2, n, 2):
        block = block_of(mask)
        piece = remote(block, block, send_sem, far_sem.at[mask // 2], partner)
        piece.wait_recv()
        remote(block, block, send_sem, near_sem, partner).start()


def arrived(blocks, sem):
    remote(blocks, blocks, sem, sem, 0).wait_recv()


def departed(blocks, sem):
    remote(blocks, blocks, sem, sem, 0).wait_send()


def tall(table):
    return table if table.shape[1] % 128 == 0 else table.T


def across(lhs, table):
    return lax.dot_general(lhs, table, (((1,), (1,)), ((), ())), preferred_element_type=F32)


def apply(lhs, table, columns):
    if columns % 128 == 0:
        return jnp.dot(lhs, table, preferred_element_type=F32)
    return across(lhs, table)


def rows_of(ref, n, start, size):
    return jnp.concatenate([ref[j, :, start : start + size].astype(F32) for j in range(n)], axis=0)


def own_columns(ref, n, me, columns):
    if columns % 128 == 0:
        at = pl.ds(pl.multiple_of(me * columns, 128), columns)
        return jnp.concatenate([ref[j, :, at].astype(F32) for j in range(n)], axis=0)
    share = 128 // columns
    at = pl.ds(pl.multiple_of(lax.div(me, share) * 128, 128), 128)
    wide = jnp.concatenate([ref[j, :, at].astype(F32) for j in range(n)], axis=0)
    part = lax.rem(me, share)
    picked = wide[:, :columns]
    for i in range(1, share):
        picked = jnp.where(part == i, wide[:, i * columns : (i + 1) * columns], picked)
    return picked


def layer_kernel(
    n, heads, key_size, value_size, names_width,
    tokens, memory, max_state, norm_gain, wv, wg, wq, wk, w_in, w_forget, forget_bias,
    head_gain, wo, expert_norm, routed, route_weights, w_gate, w_lift, w_down,
    new_memory, results, residual_out, picks_out, max_out,
    tok_s, max_s, ngain_s, v_w, g_w, q_w, k_w, in_w, forget_w, bias_s,
    hgain_s, o_w, egain_s, routed_s, rw_s, gate_w, lift_w, down_w,
    all_s, names_s, pick_s, x_s, proj_s, back_s, k_s, kt_s, v_s, c_s, w_s, mix_s,
    res_s, needed_s, own_s, owned_s, out_s,
    local_sem, mem_sem, send_sem, far_sem, near_sem, column_sem, part_sem, group_sem,
):
    me = lax.axis_index("ep")
    barrier = pltpu.get_barrier_semaphore()
    for mask in range(n - 1, 0, -1):
        pl.semaphore_signal(barrier, inc=1, device_id={"ep": flip(me, mask)})
    rows, width = tokens.shape
    most = pl.ds(0, n - 1)
    pairs = [
        (tokens, tok_s.at[:, pl.ds(0, width)]), (routed, routed_s), (norm_gain, ngain_s),
        (w_in, in_w), (w_forget, forget_w), (forget_bias, bias_s), (max_state, max_s),
        (route_weights, rw_s), (wv, v_w), (wg, g_w), (wq, q_w), (wk, k_w),
        (head_gain, hgain_s), (expert_norm, egain_s), (wo, o_w),
        (w_gate.at[0], gate_w), (w_lift.at[0], lift_w), (w_down.at[0], down_w),
    ]
    loads = [pltpu.make_async_copy(a, b, local_sem.at[i]) for i, (a, b) in enumerate(pairs)]
    for load in loads[:12]:
        load.start()

    for h in range(heads):
        for s in range(rows):
            pltpu.make_async_copy(memory.at[s, h], new_memory.at[s, h], mem_sem).start()
    for load in loads[12:]:
        load.start()

    for load in loads[:8]:
        load.wait()
    lane = lax.broadcasted_iota(jnp.int32, (rows, names_width), 1)
    which = routed_s[...]
    weights = rw_s[...]
    taken = jnp.zeros((1, names_width), F32)
    chosen = []
    named = jnp.zeros((rows, names_width), F32)
    weighed = jnp.zeros((rows, names_width), F32)
    for slot in range(SLOTS):
        for k in range(which.shape[1]):
            hit = lane == which[:, k : k + 1] + slot * n
            named = named + hit.astype(F32)
            weighed = weighed + jnp.where(hit, weights[:, k : k + 1], 0.0)
    slot_of = (lax.broadcasted_iota(jnp.int32, (1, names_width), 1) >= n).astype(F32)
    for r in range(rows):
        chosen.append(named[r : r + 1] * (taken == slot_of).astype(F32))
        taken = taken + named[r : r + 1]
    chosen = jnp.concatenate(chosen, axis=0)
    tok_s[:, width:] = chosen.astype(BF16)
    picks_out[...] = chosen * weighed

    gain = ngain_s[...]
    own = scaled_norm(tok_s[:, :width].astype(F32), gain).astype(BF16)
    input_logit = across(own, in_w[...])
    raw = across(own, forget_w[...]) + bias_s[...]
    log_forget = jnp.minimum(raw, 0.0) - jnp.log1p(jnp.exp(-jnp.abs(raw)))
    prior = log_forget + max_s[...]
    new_max = jnp.maximum(prior, input_logit)
    max_out[...] = new_max
    carried = jnp.exp(prior - new_max)
    written = jnp.exp(input_logit - new_max) * key_size**-0.5

    pl.semaphore_wait(barrier, n - 1)
    spread(n, me, tok_s, all_s.at[me], send_sem.at[0], far_sem.at[0], near_sem.at[0])
    all_s[me] = tok_s[...]
    for load in loads[8:12]:
        load.wait()
    relay(
        n, me, lambda mask: all_s.at[flip(me, mask)], send_sem.at[0], far_sem.at[0], near_sem.at[0]
    )
    arrived(all_s.at[pl.ds(0, n // 2)], near_sem.at[0])
    normed = scaled_norm(rows_of(all_s, n, 0, width), gain).astype(BF16)
    cq, cv = heads * key_size // n, heads * value_size // n
    tables = [v_w[...], g_w[...], q_w[...], k_w[...]]
    projected = jnp.concatenate(
        [apply(normed, table, c) for table, c in zip(tables, (cv, cv, cq, cq))], axis=1
    )
    for j in range(n):
        proj_s[j] = projected[j * rows : (j + 1) * rows].astype(BF16)
    per = n // heads
    exchange(
        n, me, lambda peer: proj_s.at[peer], back_s, send_sem.at[1],
        lambda mask: column_sem.at[mask // per],
    )
    back_s[me] = proj_s[me]

    columns = res_s.shape[1]
    x_s[...] = own_columns(all_s, n, me, columns)
    names_s[...] = rows_of(all_s, n, width, names_width).T
    wanted = SLOTS * n
    place = lax.broadcasted_iota(jnp.int32, (wanted, n * rows), 0)
    row = lax.broadcasted_iota(jnp.int32, (wanted, n * rows), 1)
    first = (place - place % SLOTS) // SLOTS * rows
    inside = (row >= first) & (row < first + rows)
    even = place % SLOTS == 0
    for j in range(n):
        value = jnp.where(even, names_s[j : j + 1, :], names_s[n + j : n + j + 1, :])
        pick_s[j] = jnp.where(inside, value, 0.0).astype(BF16)
    for load in loads[12:15]:
        load.wait()
    pltpu.make_async_copy(memory, new_memory, mem_sem).wait()
    for h in range(heads):
        c_s[h] = jnp.broadcast_to(carried[:, h : h + 1], (rows, value_size))
        w_s[h] = jnp.broadcast_to(written[:, h : h + 1], (rows, value_size))
    step = 32
    quarter = lax.div(me, per)
    pad = jnp.zeros((-rows % 8, key_size), F32)

    def read(h):
        pieces = [back_s[h * per + t].astype(F32) for t in range(per)]
        v = jnp.concatenate([b[:, :cv] for b in pieces], axis=1)
        g = jnp.concatenate([b[:, cv : 2 * cv] for b in pieces], axis=1)
        q = jnp.concatenate([b[:, 2 * cv : 2 * cv + cq] for b in pieces], axis=1)
        k = jnp.concatenate([b[:, 2 * cv + cq :] for b in pieces], axis=1)
        query = jnp.concatenate([q, pad], axis=0).T
        v = v * w_s[h]
        match = jnp.sum(q * k, axis=1, keepdims=True) * v
        gains = hgain_s[:, pl.ds(pl.multiple_of(h * value_size, value_size), value_size)]
        gains = gains * jax.nn.sigmoid(g)
        sums = []
        for s in range(rows):
            total = jnp.zeros((8, value_size), F32)
            for at in range(0, key_size, step):
                terms = query[at : at + step, s : s + 1] * new_memory[s, h, at : at + step, :]
                total = total + jnp.sum(terms.reshape(step // 8, 8, value_size), axis=0)
            sums.append(jnp.sum(total, axis=0, keepdims=True))
        readout = c_s[h] * jnp.concatenate(sums, axis=0) + match
        return scaled_norm(readout, gains).astype(BF16), k, v

    for i in range(heads):
        arrived(back_s.at[pl.ds(0, per if i else per - 1)], column_sem.at[i])
        h = flip(quarter, i)
        mix_s[h, me], k_s[h], v_s[h] = read(h)
        mine = mix_s.at[h, me]
        if i < heads - 1:
            spread(n, me, mine, mine, send_sem.at[2 + i], far_sem.at[1 + i], near_sem.at[1 + i])
        else:
            for mask in range(n - 1, 0, -1):
                remote(mine, mine, send_sem.at[2 + i], group_sem.at[0], flip(me, mask)).start()

    def update(h, carry):
        for s in range(rows):
            keep = c_s[h, s : s + 1, :]
            values = v_s[h, s : s + 1, :]

            def chunk(r, nothing):
                at = pl.ds(pl.multiple_of(r * step, step), step)
                new_memory[s, h, at, :] = (
                    keep * new_memory[s, h, at, :] + kt_s[h, at, s : s + 1] * values
                )
                return nothing

            lax.fori_loop(0, key_size // step, chunk, 0, unroll=True)
        return carry

    for h in range(heads):
        kt_s[h] = jnp.concatenate([k_s[h], pad], axis=0).T
    lax.fori_loop(0, heads, update, 0)
    for i in range(heads - 1):
        relay(
            n, me, lambda mask: mix_s.at[flip(quarter, mask // per ^ i), flip(me, mask)],
            send_sem.at[2 + i], far_sem.at[1 + i], near_sem.at[1 + i],
        )
    for i in range(heads - 1):
        arrived(mix_s.at[0, pl.ds(0, n // 2)], near_sem.at[1 + i])
    arrived(mix_s.at[0, most], group_sem.at[0])
    mixed = jnp.concatenate(
        [
            jnp.concatenate([mix_s[h, j].astype(F32) for j in range(n)], axis=0).astype(BF16)
            for h in range(heads)
        ],
        axis=1,
    )
    branch = apply(mixed, o_w[...], columns).astype(BF16)
    residual = (x_s[...] + branch.astype(F32)).astype(BF16)
    picked = jnp.dot(
        pick_s[...].reshape(n * wanted, n * rows), residual, preferred_element_type=F32
    ).astype(BF16)
    res_s[...] = picked
    exchange(
        n, me, lambda peer: res_s.at[pl.ds(pl.multiple_of(peer * wanted, wanted), wanted)],
        needed_s, send_sem.at[2 + heads], lambda mask: part_sem.at[mask // per],
    )
    needed_s[me] = res_s[pl.ds(pl.multiple_of(me * wanted, wanted), wanted)]
    whole = residual.astype(F32)
    for j in range(n):
        own_s[j] = whole[j * rows : (j + 1) * rows].astype(BF16)
    exchange(
        n, me, lambda peer: own_s.at[peer], owned_s, send_sem.at[3 + heads],
        lambda mask: group_sem.at[1],
    )
    owned_s[me] = own_s[me]
    for load in loads[15:]:
        load.wait()
    span = per * columns
    gate_value = jnp.zeros((wanted, gate_w.shape[1]), F32)
    lift_value = jnp.zeros((wanted, lift_w.shape[1]), F32)
    square = jnp.zeros((wanted, 1), F32)
    for i in range(heads):
        arrived(needed_s.at[pl.ds(0, per if i else per - 1)], part_sem.at[i])
        part = flip(quarter, i)
        block = jnp.concatenate([needed_s[part * per + t].astype(F32) for t in range(per)], axis=1)
        at = pl.ds(pl.multiple_of(part * span, span), span)
        square += jnp.sum(block * block, axis=1, keepdims=True)
        block = (block * egain_s[:, at]).astype(BF16)
        gate_value += jnp.dot(block, gate_w[at, :], preferred_element_type=F32)
        lift_value += jnp.dot(block, lift_w[at, :], preferred_element_type=F32)
    scale = lax.rsqrt(square / width + epsilon)
    gate_value, lift_value = gate_value * scale, lift_value * scale
    hidden = (jax.nn.silu(gate_value) * lift_value).astype(BF16)
    result = jnp.dot(hidden, down_w[...], preferred_element_type=F32)
    for j in range(n):
        out_s[j] = result[j * SLOTS : (j + 1) * SLOTS].astype(BF16)
    exchange(
        n, me, lambda peer: out_s.at[peer], results, send_sem.at[4 + heads],
        lambda mask: group_sem.at[2],
    )
    results[me] = out_s[me]
    arrived(owned_s.at[most], group_sem.at[1])
    residual_out[...] = jnp.concatenate([owned_s[j].astype(F32) for j in range(n)], axis=1)
    departed(all_s.at[most], send_sem.at[0])
    departed(proj_s.at[most], send_sem.at[1])
    for i in range(heads):
        departed(mix_s.at[0, most], send_sem.at[2 + i])
    departed(needed_s.at[most], send_sem.at[2 + heads])
    departed(own_s.at[most], send_sem.at[3 + heads])
    arrived(out_s.at[most], group_sem.at[2])
    departed(out_s.at[most], send_sem.at[4 + heads])


def combine_kernel(
    memory, results, residual, picks, new_max_in,
    layer_out, new_memory, max_out,
    out_s, top_s, mem_sem, sem,
):
    n, slots, width = results.shape
    rows, heads = new_max_in.shape

    for h in range(heads):
        for s in range(rows):
            pltpu.make_async_copy(memory.at[s, h], new_memory.at[s, h], mem_sem).start()
    top_s[...] = new_max_in[...]
    top = pltpu.make_async_copy(top_s, max_out, sem.at[0])
    top.start()
    weights = picks[...]
    total = jnp.zeros((rows, width), F32)
    for j in range(n):
        block = results[j].astype(F32)
        for s in range(slots):
            weight = weights[:, s * n + j : s * n + j + 1]
            total = total + (weight * block[s : s + 1]).astype(BF16).astype(F32)
    out_s[...] = (residual[...] + total).astype(BF16)
    out = pltpu.make_async_copy(out_s, layer_out, sem.at[1])
    out.start()
    pltpu.make_async_copy(memory, new_memory, mem_sem).wait()
    top.wait()
    out.wait()


def body(
    tokens, memory_state, max_state, norm_gain, query_weight, key_weight, value_weight,
    output_gate, input_gate, forget_gate, forget_bias, head_gain, output_weight, expert_norm,
    routed_experts, route_weights, expert_gate, expert_lift, expert_down,
):
    n = lax.axis_size("ep")
    rows, width = tokens.shape
    _, heads, key_size, value_size = memory_state.shape
    hidden = expert_gate.shape[2]
    cq, cv, columns = query_weight.shape[1], value_weight.shape[1], output_weight.shape[1]
    total_cols = 2 * cq + 2 * cv
    wv, wg, wq, wk = (tall(t) for t in (value_weight, output_gate, query_weight, key_weight))
    wo = tall(output_weight)
    names_width = -(-SLOTS * n // 128) * 128
    wanted = SLOTS * n
    sds = jax.ShapeDtypeStruct
    small = sds((rows, heads), F32)
    padded = -(-rows // 8) * 8
    new_memory, results, residual, picks, new_max = pl.pallas_call(
        functools.partial(layer_kernel, n, heads, key_size, value_size, names_width),
        out_shape=(
            pltpu.VMEM(memory_state.shape, F32),
            pltpu.VMEM((n, SLOTS, width), BF16),
            pltpu.VMEM((rows, width), F32),
            pltpu.VMEM((rows, names_width), F32),
            pltpu.VMEM((rows, heads), F32),
        ),
        in_specs=[HBM] * 19,
        out_specs=[VMEM] * 5,
        scratch_shapes=[
            pltpu.VMEM((rows, width + names_width), BF16),
            pltpu.VMEM((rows, heads), F32),
            pltpu.VMEM((1, width), F32),
            pltpu.VMEM(wv.shape, BF16),
            pltpu.VMEM(wg.shape, BF16),
            pltpu.VMEM(wq.shape, BF16),
            pltpu.VMEM(wk.shape, BF16),
            pltpu.VMEM((heads, width), BF16),
            pltpu.VMEM((heads, width), BF16),
            pltpu.VMEM((1, heads), F32),
            pltpu.VMEM((1, width), F32),
            pltpu.VMEM(wo.shape, BF16),
            pltpu.VMEM((1, width), F32),
            pltpu.VMEM(routed_experts.shape, jnp.int32),
            pltpu.VMEM(route_weights.shape, F32),
            pltpu.VMEM((width, hidden), BF16),
            pltpu.VMEM((width, hidden), BF16),
            pltpu.VMEM((hidden, width), BF16),
            pltpu.VMEM((n, rows, width + names_width), BF16),
            pltpu.VMEM((names_width, n * rows), F32),
            pltpu.VMEM((n, wanted, n * rows), BF16),
            pltpu.VMEM((n * rows, columns), F32),
            pltpu.VMEM((n, rows, total_cols), BF16),
            pltpu.VMEM((n, rows, total_cols), BF16),
            pltpu.VMEM((heads, rows, key_size), F32),
            pltpu.VMEM((heads, key_size, padded), F32),
            pltpu.VMEM((heads, rows, value_size), F32),
            pltpu.VMEM((heads, rows, value_size), F32),
            pltpu.VMEM((heads, rows, value_size), F32),
            pltpu.VMEM((heads, n, rows, value_size), BF16),
            pltpu.VMEM((n * wanted, columns), BF16),
            pltpu.VMEM((n, wanted, columns), BF16),
            pltpu.VMEM((n, rows, columns), BF16),
            pltpu.VMEM((n, rows, columns), BF16),
            pltpu.VMEM((n, SLOTS, width), BF16),
            pltpu.SemaphoreType.DMA((18,)),
            pltpu.SemaphoreType.DMA,
            pltpu.SemaphoreType.DMA((5 + heads,)),
            pltpu.SemaphoreType.DMA((heads, n // 2)),
            pltpu.SemaphoreType.DMA((heads,)),
            pltpu.SemaphoreType.DMA((heads,)),
            pltpu.SemaphoreType.DMA((heads,)),
            pltpu.SemaphoreType.DMA((3,)),
        ],
        compiler_params=pltpu.CompilerParams(
            collective_id=0, has_side_effects=True, vmem_limit_bytes=40 << 20
        ),
        name="layer",
    )(*(
        pltpu.with_memory_space_constraint(x, pltpu.HBM)
        for x in (
            tokens, memory_state, max_state, norm_gain.reshape(1, -1), wv, wg, wq, wk,
            input_gate.T, forget_gate.T, forget_bias.reshape(1, -1), head_gain.reshape(1, -1), wo,
            expert_norm.reshape(1, -1), routed_experts, route_weights,
            expert_gate, expert_lift, expert_down,
        )
    ))
    layer_out, new_memory, new_max = pl.pallas_call(
        combine_kernel,
        out_shape=(sds((rows, width), BF16), sds(memory_state.shape, F32), small),
        in_specs=[VMEM] * 5,
        out_specs=[ANY] * 3,
        scratch_shapes=[
            pltpu.VMEM((rows, width), BF16),
            pltpu.VMEM((rows, heads), F32),
            pltpu.SemaphoreType.DMA,
            pltpu.SemaphoreType.DMA((2,)),
        ],
        compiler_params=pltpu.CompilerParams(vmem_limit_bytes=8 << 20),
        name="combine",
    )(new_memory, results, residual, picks, new_max)
    return layer_out, new_memory, new_max


def solution(mesh):
    both = ("grp", "ep")
    return jax.shard_map(
        body,
        mesh=mesh,
        in_specs=(
            P(both, None), P(both, None, None, None), P(both, None), P(),
            P(None, "ep"), P(None, "ep"), P(None, "ep"), P(None, "ep"),
            P(), P(), P(), P(), P(None, "ep"), P(),
            P(both, None), P(both, None),
            P("ep", None, None), P("ep", None, None), P("ep", None, None),
        ),
        out_specs=(P(both, None), P(both, None, None, None), P(both, None)),
        check_vma=False,
    )
```

```python
import functools

import jax
import jax.numpy as jnp
from jax import lax
from jax.experimental import pallas as pl
from jax.experimental.pallas import tpu as pltpu
from jax.sharding import PartitionSpec as P

epsilon = 1e-06
F32 = jnp.float32
BF16 = jnp.bfloat16
ANY = pl.BlockSpec(memory_space=pl.ANY)
HBM = pl.BlockSpec(memory_space=pltpu.HBM)
VMEM = pl.BlockSpec(memory_space=pltpu.VMEM)
SLOTS = 2


def scaled_norm(entries, gain):
    return entries * lax.rsqrt(jnp.mean(entries * entries, axis=-1, keepdims=True) + epsilon) * gain


def flip(me, mask):
    peer, bit = me, 1
    while bit <= mask:
        if mask & bit:
            peer = peer + bit * (1 - 2 * lax.rem(lax.div(me, bit), 2))
        bit *= 2
    return peer


def remote(source, target, send_sem, recv_sem, peer):
    return pltpu.make_async_remote_copy(
        src_ref=source, dst_ref=target, send_sem=send_sem, recv_sem=recv_sem, device_id={"ep": peer}
    )


def exchange(n, me, source, landing, send_sem, recv_sem):
    for mask in range(n - 1, 0, -1):
        peer = flip(me, mask)
        remote(source(peer), landing.at[me], send_sem, recv_sem(mask), peer).start()


def landed(blocks, sem):
    pltpu.make_async_copy(blocks, blocks, sem).wait()


def spread(n, me, source, target, send_sem, far_sem, near_sem):
    for mask in [*range(n - 2, 0, -2), 1]:
        sem = near_sem if mask == 1 else far_sem.at[mask // 2 - 1]
        remote(source, target, send_sem, sem, flip(me, mask)).start()


def relay(n, me, block_of, send_sem, far_sem, near_sem):
    partner = flip(me, 1)
    for mask in range(2, n, 2):
        block = block_of(mask)
        piece = remote(block, block, send_sem, far_sem.at[mask // 2 - 1], partner)
        piece.wait_recv()
        remote(block, block, send_sem, near_sem(mask), partner).start()


def arrived(blocks, sem):
    remote(blocks, blocks, sem, sem, 0).wait_recv()


def departed(blocks, sem):
    remote(blocks, blocks, sem, sem, 0).wait_send()


def tall(table):
    return table if table.shape[1] % 128 == 0 else table.T


def across(lhs, table):
    return lax.dot_general(lhs, table, (((1,), (1,)), ((), ())), preferred_element_type=F32)


def apply(lhs, table, columns):
    if columns % 128 == 0:
        return jnp.dot(lhs, table, preferred_element_type=F32)
    return across(lhs, table)


def rows_of(ref, n, start, size):
    return jnp.concatenate([ref[j, :, start : start + size].astype(F32) for j in range(n)], axis=0)


def own_columns(ref, n, me, columns):
    if columns % 128 == 0:
        at = pl.ds(pl.multiple_of(me * columns, 128), columns)
        return jnp.concatenate([ref[j, :, at].astype(F32) for j in range(n)], axis=0)
    share = 128 // columns
    at = pl.ds(pl.multiple_of(lax.div(me, share) * 128, 128), 128)
    wide = jnp.concatenate([ref[j, :, at].astype(F32) for j in range(n)], axis=0)
    part = lax.rem(me, share)
    picked = wide[:, :columns]
    for i in range(1, share):
        picked = jnp.where(part == i, wide[:, i * columns : (i + 1) * columns], picked)
    return picked


def layer_kernel(
    n, heads, key_size, value_size, names_width,
    tokens, memory, max_state, norm_gain, wv, wg, wq, wk, w_in, w_forget, forget_bias,
    head_gain, wo, expert_norm, routed, route_weights, w_gate, w_lift, w_down,
    new_memory, results, residual_out, picks_out, max_out,
    tok_s, max_s, ngain_s, vg_w, qk_w, gates_w, bias_s,
    hgain_s, o_w, egain_s, routed_s, rw_s, up_w, down_w,
    all_s, names_s, pick_s, x_s, proj_s, back_s, kt_s, v_s, c_s, w_s, mix_s,
    res_s, needed_s, own_s, owned_s, out_s,
    local_sem, send_sem, far_sem, near_sem, column_sem, part_sem, group_sem,
):
    me = lax.axis_index("ep")
    barrier = pltpu.get_barrier_semaphore()
    for mask in range(n - 1, 0, -1):
        pl.semaphore_signal(barrier, inc=1, device_id={"ep": flip(me, mask)})
    rows, width = tokens.shape
    most = pl.ds(0, n - 1)
    cq, cv = heads * key_size // n, heads * value_size // n
    flat = cv % 128 == 0
    halves = [vg_w.at[:, pl.ds(i * cv, cv)] if flat else vg_w.at[pl.ds(i * cv, cv)] for i in range(2)]
    loads = [
        (tokens, tok_s, 0), (routed, routed_s, 1), (norm_gain, ngain_s, 2),
        (w_in, gates_w.at[0], 3), (w_forget, gates_w.at[1], 3), (forget_bias, bias_s, 4),
        (max_state, max_s, 5), (route_weights, rw_s, 6), (wv, halves[0], 7), (wg, halves[1], 7),
        (wq, qk_w.at[pl.ds(0, cq)], 8), (wk, qk_w.at[pl.ds(cq, cq)], 8),
        *(
            (memory.at[s, h], new_memory.at[s, h], 9)
            for h in range(heads) for s in range(rows)
        ),
        (head_gain, hgain_s, 10), (wo, o_w, 10 + 1), (expert_norm, egain_s, 12),
        (w_gate.at[0], up_w.at[0], 13), (w_lift.at[0], up_w.at[1], 13), (w_down.at[0], down_w, 14),
    ]
    for source, target, i in loads:
        pltpu.make_async_copy(source, target, local_sem.at[i]).start()

    for i, target in enumerate((tok_s, routed_s, ngain_s, gates_w, bias_s, max_s, rw_s)):
        landed(target, local_sem.at[i])
    lane = lax.broadcasted_iota(jnp.int32, (rows, names_width), 1)
    which = routed_s[...]
    weights = rw_s[...]
    taken = jnp.zeros((1, names_width), F32)
    chosen = []
    named = jnp.zeros((rows, names_width), F32)
    weighed = jnp.zeros((rows, names_width), F32)
    for slot in range(SLOTS):
        for k in range(which.shape[1]):
            hit = lane == which[:, k : k + 1] + slot * n
            named = named + hit.astype(F32)
            weighed = weighed + jnp.where(hit, weights[:, k : k + 1], 0.0)
    slot_of = (lax.broadcasted_iota(jnp.int32, (1, names_width), 1) >= n).astype(F32)
    for r in range(rows):
        chosen.append(named[r : r + 1] * (taken == slot_of).astype(F32))
        taken = taken + named[r : r + 1]
    chosen = jnp.concatenate(chosen, axis=0)
    for j in range(n):
        proj_s[j, :, :names_width] = chosen.astype(BF16)
    picks_out[...] = chosen * weighed

    gain = ngain_s[...]
    own = scaled_norm(tok_s[...].astype(F32), gain).astype(BF16)
    input_logit = across(own, gates_w[0])
    raw = across(own, gates_w[1]) + bias_s[...]
    log_forget = jnp.minimum(raw, 0.0) - jnp.log1p(jnp.exp(-jnp.abs(raw)))
    prior = log_forget + max_s[...]
    new_max = jnp.maximum(prior, input_logit)
    max_out[...] = new_max
    carried = jnp.exp(prior - new_max)
    written = jnp.exp(input_logit - new_max) * key_size**-0.5

    pl.semaphore_wait(barrier, n - 1)
    spread(n, me, tok_s, all_s.at[me], send_sem.at[0], far_sem.at[0], near_sem.at[0])
    all_s[me] = tok_s[...]
    landed(vg_w, local_sem.at[7])
    landed(qk_w, local_sem.at[8])
    relay(
        n, me, lambda mask: all_s.at[flip(me, mask)], send_sem.at[0], far_sem.at[0],
        lambda mask: near_sem.at[0 if mask < n // 2 else heads],
    )
    per = n // heads

    def project(origins):
        entries = jnp.concatenate([all_s[j].astype(F32) for j in origins], axis=0)
        entries = scaled_norm(entries, gain).astype(BF16)
        for table, start in ((vg_w, names_width), (qk_w, names_width + 2 * cv)):
            made = apply(entries, table[...], table.shape[1] if flat and table is vg_w else 1)
            for i, j in enumerate(origins):
                proj_s[j, :, start : start + made.shape[1]] = (
                    made[i * rows : (i + 1) * rows].astype(BF16)
                )

    def reply(masks):
        for mask in masks:
            peer = flip(me, mask)
            remote(
                proj_s.at[peer], back_s.at[me], send_sem.at[1], column_sem.at[mask // per], peer
            ).start()

    early = [*range(n // 2), *range(n // 2, n, 2)]
    late = [*range(n // 2 + 1, n, 2)]
    arrived(all_s.at[pl.ds(0, n // 4)], near_sem.at[0])
    project([flip(me, mask) for mask in early])
    reply(early[:0:-1])
    arrived(all_s.at[pl.ds(0, n // 4)], near_sem.at[heads])
    project([flip(me, mask) for mask in late])
    reply(late[::-1])
    back_s[me] = proj_s[me]

    columns = res_s.shape[1]
    x_s[...] = own_columns(all_s, n, me, columns)
    for i, target in ((10, hgain_s), (11, o_w), (12, egain_s)):
        landed(target, local_sem.at[i])
    pltpu.make_async_copy(memory, new_memory, local_sem.at[9]).wait()
    for h in range(heads):
        c_s[h] = jnp.broadcast_to(carried[:, h : h + 1], (rows, value_size))
        w_s[h] = jnp.broadcast_to(written[:, h : h + 1], (rows, value_size))
    step = 32
    quarter = lax.div(me, per)
    pad = jnp.zeros((-rows % 8, 2 * key_size), F32)

    def read(h):
        pieces = [back_s[h * per + t][:, names_width:].astype(F32) for t in range(per)]
        v = jnp.concatenate([b[:, :cv] for b in pieces], axis=1)
        g = jnp.concatenate([b[:, cv : 2 * cv] for b in pieces], axis=1)
        qk = jnp.concatenate([b[:, 2 * cv :] for b in pieces], axis=1)
        turned = jnp.concatenate([qk, pad], axis=0).T
        query = jnp.concatenate([turned[t * 2 * cq : t * 2 * cq + cq] for t in range(per)], axis=0)
        key = jnp.concatenate([turned[t * 2 * cq + cq : (t + 1) * 2 * cq] for t in range(per)], axis=0)
        v = v * w_s[h]
        match = jnp.sum(query * key, axis=0, keepdims=True)
        gains = hgain_s[:, pl.ds(pl.multiple_of(h * value_size, value_size), value_size)]
        gains = gains * jax.nn.sigmoid(g)
        sums, own_match = [], []
        for s in range(rows):
            total = jnp.zeros((8, value_size), F32)
            for at in range(0, key_size, step):
                terms = query[at : at + step, s : s + 1] * new_memory[s, h, at : at + step, :]
                total = total + jnp.sum(terms.reshape(step // 8, 8, value_size), axis=0)
            sums.append(jnp.sum(total, axis=0, keepdims=True))
            own_match.append(match[:, s : s + 1] * v[s : s + 1])
        readout = c_s[h] * jnp.concatenate(sums, axis=0) + jnp.concatenate(own_match, axis=0)
        return scaled_norm(readout, gains).astype(BF16), key, v

    for i in range(heads):
        arrived(back_s.at[pl.ds(0, per if i else per - 1)], column_sem.at[i])
        h = flip(quarter, i)
        mix_s[h, me], kt_s[h], v_s[h] = read(h)
        mine = mix_s.at[h, me]
        if i < heads - 1:
            spread(n, me, mine, mine, send_sem.at[2 + i], far_sem.at[1 + i], near_sem.at[1 + i])
        else:
            for mask in range(n - 1, 0, -1):
                remote(mine, mine, send_sem.at[2 + i], group_sem.at[0], flip(me, mask)).start()
    names_s[...] = rows_of(back_s, n, 0, names_width).T
    wanted = SLOTS * n
    place = lax.broadcasted_iota(jnp.int32, (wanted, n * rows), 0)
    row = lax.broadcasted_iota(jnp.int32, (wanted, n * rows), 1)
    first = (place - place % SLOTS) // SLOTS * rows
    inside = (row >= first) & (row < first + rows)
    even = place % SLOTS == 0
    for j in range(n):
        value = jnp.where(even, names_s[j : j + 1, :], names_s[n + j : n + j + 1, :])
        pick_s[j] = jnp.where(inside, value, 0.0).astype(BF16)

    def update(h, carry):
        for s in range(rows):
            keep = c_s[h, s : s + 1, :]
            values = v_s[h, s : s + 1, :]

            def chunk(r, nothing):
                at = pl.ds(pl.multiple_of(r * step, step), step)
                new_memory[s, h, at, :] = (
                    keep * new_memory[s, h, at, :] + kt_s[h, at, s : s + 1] * values
                )
                return nothing

            lax.fori_loop(0, key_size // step, chunk, 0, unroll=True)
        return carry

    lax.fori_loop(0, heads, update, 0)
    for i in range(heads - 1):
        relay(
            n, me, lambda mask: mix_s.at[flip(quarter, mask // per ^ i), flip(me, mask)],
            send_sem.at[2 + i], far_sem.at[1 + i], lambda mask: near_sem.at[1 + i],
        )
    for i in range(heads - 1):
        arrived(mix_s.at[0, pl.ds(0, n // 2)], near_sem.at[1 + i])
    arrived(mix_s.at[0, most], group_sem.at[0])
    mixed = jnp.concatenate(
        [
            jnp.concatenate([mix_s[h, j].astype(F32) for j in range(n)], axis=0).astype(BF16)
            for h in range(heads)
        ],
        axis=1,
    )
    branch = apply(mixed, o_w[...], columns).astype(BF16)
    residual = (x_s[...] + branch.astype(F32)).astype(BF16)
    picked = jnp.dot(
        pick_s[...].reshape(n * wanted, n * rows), residual, preferred_element_type=F32
    ).astype(BF16)
    res_s[...] = picked
    exchange(
        n, me, lambda peer: res_s.at[pl.ds(pl.multiple_of(peer * wanted, wanted), wanted)],
        needed_s, send_sem.at[2 + heads], lambda mask: part_sem.at[mask // per],
    )
    needed_s[me] = res_s[pl.ds(pl.multiple_of(me * wanted, wanted), wanted)]
    whole = residual.astype(F32)
    for j in range(n):
        own_s[j] = whole[j * rows : (j + 1) * rows].astype(BF16)
    owned_s[me] = own_s[me]
    landed(up_w, local_sem.at[13])
    landed(down_w, local_sem.at[14])
    span = per * columns
    gate_value = jnp.zeros((wanted, up_w.shape[2]), F32)
    lift_value = jnp.zeros((wanted, up_w.shape[2]), F32)
    square = jnp.zeros((wanted, 1), F32)
    for i in range(heads):
        arrived(needed_s.at[pl.ds(0, per if i else per - 1)], part_sem.at[i])
        if i == heads - 2:
            exchange(
                n, me, lambda peer: own_s.at[peer], owned_s, send_sem.at[3 + heads],
                lambda mask: group_sem.at[1],
            )
        part = flip(quarter, i)
        block = jnp.concatenate([needed_s[part * per + t].astype(F32) for t in range(per)], axis=1)
        at = pl.ds(pl.multiple_of(part * span, span), span)
        square += jnp.sum(block * block, axis=1, keepdims=True)
        block = (block * egain_s[:, at]).astype(BF16)
        gate_value += jnp.dot(block, up_w[0, at, :], preferred_element_type=F32)
        lift_value += jnp.dot(block, up_w[1, at, :], preferred_element_type=F32)
    scale = lax.rsqrt(square / width + epsilon)
    gate_value, lift_value = gate_value * scale, lift_value * scale
    hidden = (jax.nn.silu(gate_value) * lift_value).astype(BF16)
    result = jnp.dot(hidden, down_w[...], preferred_element_type=F32)
    for j in range(n):
        out_s[j] = result[j * SLOTS : (j + 1) * SLOTS].astype(BF16)
    exchange(
        n, me, lambda peer: out_s.at[peer], results, send_sem.at[4 + heads],
        lambda mask: group_sem.at[2],
    )
    results[me] = out_s[me]
    arrived(owned_s.at[most], group_sem.at[1])
    residual_out[...] = jnp.concatenate([owned_s[j].astype(F32) for j in range(n)], axis=1)
    departed(all_s.at[most], send_sem.at[0])
    departed(proj_s.at[most], send_sem.at[1])
    for i in range(heads):
        departed(mix_s.at[0, most], send_sem.at[2 + i])
    departed(needed_s.at[most], send_sem.at[2 + heads])
    departed(own_s.at[most], send_sem.at[3 + heads])
    arrived(out_s.at[most], group_sem.at[2])
    departed(out_s.at[most], send_sem.at[4 + heads])


def combine_kernel(
    memory, results, residual, picks, new_max_in,
    layer_out, new_memory, max_out,
    out_s, top_s, mem_sem, sem,
):
    n, slots, width = results.shape
    rows, heads = new_max_in.shape

    for h in range(heads):
        for s in range(rows):
            for at in range(0, memory.shape[2], memory.shape[2] // 4):
                block = (s, h, pl.ds(at, memory.shape[2] // 4))
                pltpu.make_async_copy(memory.at[block], new_memory.at[block], mem_sem).start()
    top_s[...] = new_max_in[...]
    top = pltpu.make_async_copy(top_s, max_out, sem.at[0])
    top.start()
    weights = picks[...]
    total = jnp.zeros((rows, width), F32)
    for j in range(n):
        block = results[j].astype(F32)
        for s in range(slots):
            weight = weights[:, s * n + j : s * n + j + 1]
            total = total + (weight * block[s : s + 1]).astype(BF16).astype(F32)
    out_s[...] = (residual[...] + total).astype(BF16)
    out = pltpu.make_async_copy(out_s, layer_out, sem.at[1])
    out.start()
    pltpu.make_async_copy(memory, new_memory, mem_sem).wait()
    top.wait()
    out.wait()


def body(
    tokens, memory_state, max_state, norm_gain, query_weight, key_weight, value_weight,
    output_gate, input_gate, forget_gate, forget_bias, head_gain, output_weight, expert_norm,
    routed_experts, route_weights, expert_gate, expert_lift, expert_down,
):
    n = lax.axis_size("ep")
    rows, width = tokens.shape
    _, heads, key_size, value_size = memory_state.shape
    hidden = expert_gate.shape[2]
    cq, cv, columns = query_weight.shape[1], value_weight.shape[1], output_weight.shape[1]
    wv, wg, wo = tall(value_weight), tall(output_gate), tall(output_weight)
    wq, wk = query_weight.T, key_weight.T
    vg_shape = (width, 2 * cv) if wv.shape[0] == width and cv % 128 == 0 else (2 * cv, width)
    names_width = -(-SLOTS * n // 128) * 128
    total_cols = names_width + 2 * cq + 2 * cv
    wanted = SLOTS * n
    sds = jax.ShapeDtypeStruct
    small = sds((rows, heads), F32)
    padded = -(-rows // 8) * 8
    new_memory, results, residual, picks, new_max = pl.pallas_call(
        functools.partial(layer_kernel, n, heads, key_size, value_size, names_width),
        out_shape=(
            pltpu.VMEM(memory_state.shape, F32),
            pltpu.VMEM((n, SLOTS, width), BF16),
            pltpu.VMEM((rows, width), F32),
            pltpu.VMEM((rows, names_width), F32),
            pltpu.VMEM((rows, heads), F32),
        ),
        in_specs=[HBM] * 19,
        out_specs=[VMEM] * 5,
        scratch_shapes=[
            pltpu.VMEM((rows, width), BF16),
            pltpu.VMEM((rows, heads), F32),
            pltpu.VMEM((1, width), F32),
            pltpu.VMEM(vg_shape, BF16),
            pltpu.VMEM((2 * cq, width), BF16),
            pltpu.VMEM((2, heads, width), BF16),
            pltpu.VMEM((1, heads), F32),
            pltpu.VMEM((1, width), F32),
            pltpu.VMEM(wo.shape, BF16),
            pltpu.VMEM((1, width), F32),
            pltpu.VMEM(routed_experts.shape, jnp.int32),
            pltpu.VMEM(route_weights.shape, F32),
            pltpu.VMEM((2, width, hidden), BF16),
            pltpu.VMEM((hidden, width), BF16),
            pltpu.VMEM((n, rows, width), BF16),
            pltpu.VMEM((names_width, n * rows), F32),
            pltpu.VMEM((n, wanted, n * rows), BF16),
            pltpu.VMEM((n * rows, columns), F32),
            pltpu.VMEM((n, rows, total_cols), BF16),
            pltpu.VMEM((n, rows, total_cols), BF16),
            pltpu.VMEM((heads, key_size, padded), F32),
            pltpu.VMEM((heads, rows, value_size), F32),
            pltpu.VMEM((heads, rows, value_size), F32),
            pltpu.VMEM((heads, rows, value_size), F32),
            pltpu.VMEM((heads, n, rows, value_size), BF16),
            pltpu.VMEM((n * wanted, columns), BF16),
            pltpu.VMEM((n, wanted, columns), BF16),
            pltpu.VMEM((n, rows, columns), BF16),
            pltpu.VMEM((n, rows, columns), BF16),
            pltpu.VMEM((n, SLOTS, width), BF16),
            pltpu.SemaphoreType.DMA((15,)),
            pltpu.SemaphoreType.DMA((5 + heads,)),
            pltpu.SemaphoreType.DMA((heads, n // 2 - 1)),
            pltpu.SemaphoreType.DMA((heads + 1,)),
            pltpu.SemaphoreType.DMA((heads,)),
            pltpu.SemaphoreType.DMA((heads,)),
            pltpu.SemaphoreType.DMA((3,)),
        ],
        compiler_params=pltpu.CompilerParams(
            collective_id=0, has_side_effects=True, vmem_limit_bytes=40 << 20
        ),
        name="layer",
    )(*(
        pltpu.with_memory_space_constraint(x, pltpu.HBM)
        for x in (
            tokens, memory_state, max_state, norm_gain.reshape(1, -1), wv, wg, wq, wk,
            input_gate.T, forget_gate.T, forget_bias.reshape(1, -1), head_gain.reshape(1, -1), wo,
            expert_norm.reshape(1, -1), routed_experts, route_weights,
            expert_gate, expert_lift, expert_down,
        )
    ))
    layer_out, new_memory, new_max = pl.pallas_call(
        combine_kernel,
        out_shape=(sds((rows, width), BF16), sds(memory_state.shape, F32), small),
        in_specs=[VMEM] * 5,
        out_specs=[ANY] * 3,
        scratch_shapes=[
            pltpu.VMEM((rows, width), BF16),
            pltpu.VMEM((rows, heads), F32),
            pltpu.SemaphoreType.DMA,
            pltpu.SemaphoreType.DMA((2,)),
        ],
        compiler_params=pltpu.CompilerParams(vmem_limit_bytes=8 << 20),
        name="combine",
    )(new_memory, results, residual, picks, new_max)
    return layer_out, new_memory, new_max


def solution(mesh):
    both = ("grp", "ep")
    return jax.shard_map(
        body,
        mesh=mesh,
        in_specs=(
            P(both, None), P(both, None, None, None), P(both, None), P(),
            P(None, "ep"), P(None, "ep"), P(None, "ep"), P(None, "ep"),
            P(), P(), P(), P(), P(None, "ep"), P(),
            P(both, None), P(both, None),
            P("ep", None, None), P("ep", None, None), P("ep", None, None),
        ),
        out_specs=(P(both, None), P(both, None, None, None), P(both, None)),
        check_vma=False,
    )
```

```python
import functools

import jax
import jax.numpy as jnp
from jax import lax
from jax.experimental import pallas as pl
from jax.experimental.pallas import tpu as pltpu
from jax.sharding import PartitionSpec as P

epsilon = 1e-06
F32 = jnp.float32
BF16 = jnp.bfloat16
ANY = pl.BlockSpec(memory_space=pl.ANY)
HBM = pl.BlockSpec(memory_space=pltpu.HBM)
VMEM = pl.BlockSpec(memory_space=pltpu.VMEM)
SLOTS = 2


def scaled_norm(entries, gain):
    return entries * lax.rsqrt(jnp.mean(entries * entries, axis=-1, keepdims=True) + epsilon) * gain


def flip(me, mask):
    peer, bit = me, 1
    while bit <= mask:
        if mask & bit:
            peer = peer + bit * (1 - 2 * lax.rem(lax.div(me, bit), 2))
        bit *= 2
    return peer


def remote(source, target, send_sem, recv_sem, peer):
    return pltpu.make_async_remote_copy(
        src_ref=source, dst_ref=target, send_sem=send_sem, recv_sem=recv_sem, device_id={"ep": peer}
    )


def exchange(n, me, source, landing, send_sem, recv_sem):
    for mask in range(n - 1, 0, -1):
        peer = flip(me, mask)
        remote(source(peer), landing.at[me], send_sem, recv_sem(mask), peer).start()


def landed(blocks, sem):
    pltpu.make_async_copy(blocks, blocks, sem).wait()


def spread(n, me, source, target, send_sem, recv_sem):
    for mask in range(n - 2, 0, -2):
        remote(source(mask), target, send_sem, recv_sem(mask), flip(me, mask)).start()


def arrived(blocks, sem):
    remote(blocks, blocks, sem, sem, 0).wait_recv()


def departed(blocks, sem):
    remote(blocks, blocks, sem, sem, 0).wait_send()


def tall(table):
    return table if table.shape[1] % 128 == 0 else table.T


def across(lhs, table):
    return lax.dot_general(lhs, table, (((1,), (1,)), ((), ())), preferred_element_type=F32)


def apply(lhs, table):
    if table.shape[0] == lhs.shape[1]:
        return jnp.dot(lhs, table, preferred_element_type=F32)
    return across(lhs, table)


def rows_of(ref, n, start, size):
    return jnp.concatenate([ref[j, :, start : start + size].astype(F32) for j in range(n)], axis=0)


def layer_kernel(
    n, heads, key_size, value_size, names_width,
    tokens, memory, max_state, norm_gain, wv, wg, wq, wk, w_in, w_forget, forget_bias,
    head_gain, wo, expert_norm, routed, route_weights, w_gate, w_lift, w_down,
    new_memory, results, residual_out, picks_out, max_out,
    tok_s, max_s, ngain_s, vg_w, qk_w, gates_w, bias_s,
    hgain_s, o_w, egain_s, routed_s, rw_s, up_w, down_w,
    all_s, names_s, pick_s, x_s, proj_s, back_s, kt_s, v_s, c_s, w_s, mix_s,
    res_s, needed_s, own_s, owned_s, out_s,
    local_sem, send_sem, column_sem, part_sem, group_sem,
):
    me = lax.axis_index("ep")
    barrier = pltpu.get_barrier_semaphore()
    for mask in range(n - 1, 0, -1):
        pl.semaphore_signal(barrier, inc=1, device_id={"ep": flip(me, mask)})
    rows, width = tokens.shape
    most, same = pl.ds(0, n - 1), pl.ds(0, n // 2 - 1)
    core, chip = lax.rem(me, 2), lax.div(me, 2)
    cq, cv = heads * key_size // n, heads * value_size // n
    columns = wo.shape[1] if wo.shape[0] == width else wo.shape[0]

    def part_of(table, size, start, count):
        at = pl.ds(pl.multiple_of(core * size, size) + start, count)
        return table.at[:, at] if table.shape[0] == width else table.at[at]

    shared = [
        part_of(vg_w, 2 * cv, 0, 2 * cv), part_of(qk_w, 2 * cq, 0, 2 * cq),
        part_of(o_w, columns, 0, columns),
    ]
    loads = [
        (tokens, tok_s, 0), (routed, routed_s, 1), (norm_gain, ngain_s, 2),
        (w_in, gates_w.at[0], 3), (w_forget, gates_w.at[1], 3), (forget_bias, bias_s, 4),
        (max_state, max_s, 5), (route_weights, rw_s, 6), (wv, part_of(vg_w, 2 * cv, 0, cv), 7),
        (wg, part_of(vg_w, 2 * cv, cv, cv), 7),
        (wq, part_of(qk_w, 2 * cq, 0, cq), 8),
        (wk, part_of(qk_w, 2 * cq, cq, cq), 8), (wo, shared[2], 10 + 1),
        *(
            (memory.at[s, h], new_memory.at[s, h], 9)
            for h in range(heads) for s in range(rows)
        ),
        (head_gain, hgain_s, 10), (expert_norm, egain_s, 12),
        (w_gate.at[0], up_w.at[0], 13), (w_lift.at[0], up_w.at[1], 13), (w_down.at[0], down_w, 14),
    ]
    for source, target, i in loads:
        pltpu.make_async_copy(source, target, local_sem.at[i]).start()

    for i, target in enumerate((tok_s, routed_s, ngain_s, gates_w, bias_s, max_s, rw_s)):
        landed(target, local_sem.at[i])
    lane = lax.broadcasted_iota(jnp.int32, (rows, names_width), 1)
    which = routed_s[...]
    weights = rw_s[...]
    taken = jnp.zeros((1, names_width), F32)
    chosen = []
    named = jnp.zeros((rows, names_width), F32)
    weighed = jnp.zeros((rows, names_width), F32)
    for slot in range(SLOTS):
        for k in range(which.shape[1]):
            hit = lane == which[:, k : k + 1] + slot * n
            named = named + hit.astype(F32)
            weighed = weighed + jnp.where(hit, weights[:, k : k + 1], 0.0)
    slot_of = (lax.broadcasted_iota(jnp.int32, (1, names_width), 1) >= n).astype(F32)
    for r in range(rows):
        chosen.append(named[r : r + 1] * (taken == slot_of).astype(F32))
        taken = taken + named[r : r + 1]
    chosen = jnp.concatenate(chosen, axis=0)
    for t in range(n // 2):
        for c in range(2):
            proj_s[t, c, :, :names_width] = chosen.astype(BF16)
    picks_out[...] = chosen * weighed

    gain = ngain_s[...]
    own = scaled_norm(tok_s[...].astype(F32), gain).astype(BF16)
    input_logit = across(own, gates_w[0])
    raw = across(own, gates_w[1]) + bias_s[...]
    log_forget = jnp.minimum(raw, 0.0) - jnp.log1p(jnp.exp(-jnp.abs(raw)))
    prior = log_forget + max_s[...]
    new_max = jnp.maximum(prior, input_logit)
    max_out[...] = new_max
    carried = jnp.exp(prior - new_max)
    written = jnp.exp(input_logit - new_max) * key_size**-0.5

    pl.semaphore_wait(barrier, n - 1)
    spread(n, me, lambda mask: tok_s, all_s.at[chip], send_sem.at[0], lambda mask: group_sem.at[0])
    all_s[chip] = tok_s[...]
    partner = flip(me, 1)
    for i, block in enumerate(shared):
        landed(block, local_sem.at[(7, 8, 11)[i]])
        remote(block, block, send_sem.at[5 + heads + i], group_sem.at[3 + i], partner).start()
    per = n // heads
    arrived(shared[0], group_sem.at[3])
    arrived(shared[1], group_sem.at[4])
    arrived(all_s.at[same], group_sem.at[0])
    entries = jnp.concatenate([all_s[t].astype(F32) for t in range(n // 2)], axis=0)
    entries = scaled_norm(entries, gain).astype(BF16)
    for table, start, size in ((vg_w, names_width, 2 * cv), (qk_w, names_width + 2 * cv, 2 * cq)):
        made = apply(entries, table[...]).astype(BF16).astype(F32)
        for t in range(n // 2):
            for c in range(2):
                proj_s[t, c, :, start : start + size] = (
                    made[t * rows : (t + 1) * rows, c * size : (c + 1) * size].astype(BF16)
                )
    spread(
        n, me, lambda mask: proj_s.at[flip(chip, mask // 2)], back_s.at[chip], send_sem.at[1],
        lambda mask: column_sem.at[mask // per],
    )
    back_s[chip] = proj_s[chip]

    at = pl.ds(pl.multiple_of(chip * 2 * columns, 2 * columns), 2 * columns)
    x_s[...] = jnp.concatenate([all_s[t, :, at].astype(F32) for t in range(n // 2)], axis=0)
    for i, target in ((10, hgain_s), (12, egain_s)):
        landed(target, local_sem.at[i])
    pltpu.make_async_copy(memory, new_memory, local_sem.at[9]).wait()
    for h in range(heads):
        c_s[h] = jnp.broadcast_to(carried[:, h : h + 1], (rows, value_size))
        w_s[h] = jnp.broadcast_to(written[:, h : h + 1], (rows, value_size))
    step = 32
    quarter = lax.div(me, per)
    pad = jnp.zeros((-rows % 8, 2 * key_size), F32)

    def read(h):
        pieces = [
            back_s[h * (per // 2) + t // 2, t % 2][:, names_width:].astype(F32) for t in range(per)
        ]
        v = jnp.concatenate([b[:, :cv] for b in pieces], axis=1)
        g = jnp.concatenate([b[:, cv : 2 * cv] for b in pieces], axis=1)
        qk = jnp.concatenate([b[:, 2 * cv :] for b in pieces], axis=1)
        turned = jnp.concatenate([qk, pad], axis=0).T
        query = jnp.concatenate([turned[t * 2 * cq : t * 2 * cq + cq] for t in range(per)], axis=0)
        key = jnp.concatenate([turned[t * 2 * cq + cq : (t + 1) * 2 * cq] for t in range(per)], axis=0)
        v = v * w_s[h]
        match = jnp.sum(query * key, axis=0, keepdims=True)
        gains = hgain_s[:, pl.ds(pl.multiple_of(h * value_size, value_size), value_size)]
        gains = gains * jax.nn.sigmoid(g)
        sums, own_match = [], []
        for s in range(rows):
            total = jnp.zeros((8, value_size), F32)
            for at in range(0, key_size, step):
                terms = query[at : at + step, s : s + 1] * new_memory[s, h, at : at + step, :]
                total = total + jnp.sum(terms.reshape(step // 8, 8, value_size), axis=0)
            sums.append(jnp.sum(total, axis=0, keepdims=True))
            own_match.append(match[:, s : s + 1] * v[s : s + 1])
        readout = c_s[h] * jnp.concatenate(sums, axis=0) + jnp.concatenate(own_match, axis=0)
        return scaled_norm(readout, gains).astype(BF16), key, v

    for i in range(heads):
        count = per // 2 if i else per // 2 - 1
        if count:
            arrived(back_s.at[pl.ds(0, count)], column_sem.at[i])
        h = flip(quarter, i)
        mix_s[h, chip], kt_s[h], v_s[h] = read(h)
        mine = mix_s.at[h, chip]
        spread(n, me, lambda mask: mine, mine, send_sem.at[2], lambda mask: group_sem.at[6])
    names_s[...] = jnp.concatenate(
        [back_s[t, 0][:, :names_width].astype(F32) for t in range(n // 2)], axis=0
    ).T
    wanted = SLOTS * n // 2
    place = lax.broadcasted_iota(jnp.int32, (wanted, n // 2 * rows), 0)
    row = lax.broadcasted_iota(jnp.int32, (wanted, n // 2 * rows), 1)
    first = (place - place % SLOTS) // SLOTS * rows
    inside = (row >= first) & (row < first + rows)
    even = place % SLOTS == 0
    for j in range(n):
        value = jnp.where(even, names_s[j : j + 1, :], names_s[n + j : n + j + 1, :])
        pick_s[j] = jnp.where(inside, value, 0.0).astype(BF16)

    def update(h, carry):
        for s in range(rows):
            keep = c_s[h, s : s + 1, :]
            values = v_s[h, s : s + 1, :]

            def chunk(r, nothing):
                at = pl.ds(pl.multiple_of(r * step, step), step)
                new_memory[s, h, at, :] = (
                    keep * new_memory[s, h, at, :] + kt_s[h, at, s : s + 1] * values
                )
                return nothing

            lax.fori_loop(0, key_size // step, chunk, 0, unroll=True)
        return carry

    lax.fori_loop(0, heads, update, 0)
    arrived(mix_s.at[:, same], group_sem.at[6])
    arrived(shared[2], group_sem.at[5])
    mixed = jnp.concatenate(
        [
            jnp.concatenate([mix_s[h, t].astype(F32) for t in range(n // 2)], axis=0).astype(BF16)
            for h in range(heads)
        ],
        axis=1,
    )
    branch = apply(mixed, o_w[...]).astype(BF16)
    residual = (x_s[...] + branch.astype(F32)).astype(BF16)
    picked = jnp.dot(
        pick_s[...].reshape(n * wanted, n // 2 * rows), residual, preferred_element_type=F32
    ).astype(BF16)
    res_s[...] = picked
    exchange(
        n, me, lambda peer: res_s.at[pl.ds(pl.multiple_of(peer * wanted, wanted), wanted)],
        needed_s, send_sem.at[2 + heads], lambda mask: part_sem.at[mask // per],
    )
    needed_s[me] = res_s[pl.ds(pl.multiple_of(me * wanted, wanted), wanted)]
    whole = residual.astype(F32)
    for t in range(n // 2):
        own_s[t] = whole[t * rows : (t + 1) * rows].astype(BF16)
    owned_s[chip] = own_s[chip]
    landed(up_w, local_sem.at[13])
    landed(down_w, local_sem.at[14])
    span = per * columns
    gate_value = jnp.zeros((2 * wanted, up_w.shape[2]), F32)
    lift_value = jnp.zeros((2 * wanted, up_w.shape[2]), F32)
    square = jnp.zeros((2 * wanted, 1), F32)
    for i in range(heads):
        arrived(needed_s.at[pl.ds(0, per if i else per - 1)], part_sem.at[i])
        if i == heads - 2:
            spread(
                n, me, lambda mask: own_s.at[flip(chip, mask // 2)], owned_s.at[chip],
                send_sem.at[3 + heads], lambda mask: group_sem.at[1],
            )
        part = flip(quarter, i)
        block = jnp.concatenate(
            [
                jnp.concatenate(
                    [needed_s[part * per + t + c].astype(F32) for t in range(0, per, 2)], axis=1
                )
                for c in range(2)
            ],
            axis=0,
        )
        at = pl.ds(pl.multiple_of(part * span, span), span)
        square += jnp.sum(block * block, axis=1, keepdims=True)
        block = (block * egain_s[:, at]).astype(BF16)
        gate_value += jnp.dot(block, up_w[0, at, :], preferred_element_type=F32)
        lift_value += jnp.dot(block, up_w[1, at, :], preferred_element_type=F32)
    scale = lax.rsqrt(square / width + epsilon)
    gate_value, lift_value = gate_value * scale, lift_value * scale
    hidden = (jax.nn.silu(gate_value) * lift_value).astype(BF16)
    result = jnp.dot(hidden, down_w[...], preferred_element_type=F32)
    for j in range(n):
        at = j % 2 * wanted + j // 2 * SLOTS
        out_s[j] = result[at : at + SLOTS].astype(BF16)
    exchange(
        n, me, lambda peer: out_s.at[peer], results, send_sem.at[4 + heads],
        lambda mask: group_sem.at[2],
    )
    results[me] = out_s[me]
    arrived(owned_s.at[same], group_sem.at[1])
    residual_out[...] = jnp.concatenate([owned_s[t].astype(F32) for t in range(n // 2)], axis=1)
    departed(all_s.at[same], send_sem.at[0])
    departed(proj_s.at[same], send_sem.at[1])
    departed(mix_s.at[:, same], send_sem.at[2])
    for i, block in enumerate(shared):
        departed(block, send_sem.at[5 + heads + i])
    departed(needed_s.at[most], send_sem.at[2 + heads])
    departed(own_s.at[same], send_sem.at[3 + heads])
    arrived(out_s.at[most], group_sem.at[2])
    departed(out_s.at[most], send_sem.at[4 + heads])


def combine_kernel(
    memory, results, residual, picks, new_max_in,
    layer_out, new_memory, max_out,
    out_s, top_s, mem_sem, sem,
):
    n, slots, width = results.shape
    rows, heads = new_max_in.shape

    for h in range(heads):
        for s in range(rows):
            for at in range(0, memory.shape[2], memory.shape[2] // 4):
                block = (s, h, pl.ds(at, memory.shape[2] // 4))
                pltpu.make_async_copy(memory.at[block], new_memory.at[block], mem_sem).start()
    top_s[...] = new_max_in[...]
    top = pltpu.make_async_copy(top_s, max_out, sem.at[0])
    top.start()
    weights = picks[...]
    total = jnp.zeros((rows, width), F32)
    for j in range(n):
        block = results[j].astype(F32)
        for s in range(slots):
            weight = weights[:, s * n + j : s * n + j + 1]
            total = total + (weight * block[s : s + 1]).astype(BF16).astype(F32)
    out_s[...] = (residual[...] + total).astype(BF16)
    out = pltpu.make_async_copy(out_s, layer_out, sem.at[1])
    out.start()
    pltpu.make_async_copy(memory, new_memory, mem_sem).wait()
    top.wait()
    out.wait()


def body(
    tokens, memory_state, max_state, norm_gain, query_weight, key_weight, value_weight,
    output_gate, input_gate, forget_gate, forget_bias, head_gain, output_weight, expert_norm,
    routed_experts, route_weights, expert_gate, expert_lift, expert_down,
):
    n = lax.axis_size("ep")
    rows, width = tokens.shape
    _, heads, key_size, value_size = memory_state.shape
    hidden = expert_gate.shape[2]
    cq, cv, columns = query_weight.shape[1], value_weight.shape[1], output_weight.shape[1]
    wv, wg, wo = tall(value_weight), tall(output_gate), tall(output_weight)
    wq, wk = query_weight.T, key_weight.T
    vg_shape = (width, 4 * cv) if cv % 128 == 0 else (4 * cv, width)
    o_shape = (width, 2 * columns) if columns % 128 == 0 else (2 * columns, width)
    names_width = -(-SLOTS * n // 128) * 128
    total_cols = names_width + 2 * cq + 2 * cv
    wanted = SLOTS * n // 2
    sds = jax.ShapeDtypeStruct
    small = sds((rows, heads), F32)
    padded = -(-rows // 8) * 8
    new_memory, results, residual, picks, new_max = pl.pallas_call(
        functools.partial(layer_kernel, n, heads, key_size, value_size, names_width),
        out_shape=(
            pltpu.VMEM(memory_state.shape, F32),
            pltpu.VMEM((n, SLOTS, width), BF16),
            pltpu.VMEM((rows, width), F32),
            pltpu.VMEM((rows, names_width), F32),
            pltpu.VMEM((rows, heads), F32),
        ),
        in_specs=[HBM] * 19,
        out_specs=[VMEM] * 5,
        scratch_shapes=[
            pltpu.VMEM((rows, width), BF16),
            pltpu.VMEM((rows, heads), F32),
            pltpu.VMEM((1, width), F32),
            pltpu.VMEM(vg_shape, BF16),
            pltpu.VMEM((4 * cq, width), BF16),
            pltpu.VMEM((2, heads, width), BF16),
            pltpu.VMEM((1, heads), F32),
            pltpu.VMEM((1, width), F32),
            pltpu.VMEM(o_shape, BF16),
            pltpu.VMEM((1, width), F32),
            pltpu.VMEM(routed_experts.shape, jnp.int32),
            pltpu.VMEM(route_weights.shape, F32),
            pltpu.VMEM((2, width, hidden), BF16),
            pltpu.VMEM((hidden, width), BF16),
            pltpu.VMEM((n // 2, rows, width), BF16),
            pltpu.VMEM((names_width, n // 2 * rows), F32),
            pltpu.VMEM((n, wanted, n // 2 * rows), BF16),
            pltpu.VMEM((n // 2 * rows, 2 * columns), F32),
            pltpu.VMEM((n // 2, 2, rows, total_cols), BF16),
            pltpu.VMEM((n // 2, 2, rows, total_cols), BF16),
            pltpu.VMEM((heads, key_size, padded), F32),
            pltpu.VMEM((heads, rows, value_size), F32),
            pltpu.VMEM((heads, rows, value_size), F32),
            pltpu.VMEM((heads, rows, value_size), F32),
            pltpu.VMEM((heads, n // 2, rows, value_size), BF16),
            pltpu.VMEM((n * wanted, 2 * columns), BF16),
            pltpu.VMEM((n, wanted, 2 * columns), BF16),
            pltpu.VMEM((n // 2, rows, 2 * columns), BF16),
            pltpu.VMEM((n // 2, rows, 2 * columns), BF16),
            pltpu.VMEM((n, SLOTS, width), BF16),
            pltpu.SemaphoreType.DMA((15,)),
            pltpu.SemaphoreType.DMA((8 + heads,)),
            pltpu.SemaphoreType.DMA((heads,)),
            pltpu.SemaphoreType.DMA((heads,)),
            pltpu.SemaphoreType.DMA((7,)),
        ],
        compiler_params=pltpu.CompilerParams(
            collective_id=0, has_side_effects=True, vmem_limit_bytes=40 << 20
        ),
        name="layer",
    )(*(
        pltpu.with_memory_space_constraint(x, pltpu.HBM)
        for x in (
            tokens, memory_state, max_state, norm_gain.reshape(1, -1), wv, wg, wq, wk,
            input_gate.T, forget_gate.T, forget_bias.reshape(1, -1), head_gain.reshape(1, -1), wo,
            expert_norm.reshape(1, -1), routed_experts, route_weights,
            expert_gate, expert_lift, expert_down,
        )
    ))
    layer_out, new_memory, new_max = pl.pallas_call(
        combine_kernel,
        out_shape=(sds((rows, width), BF16), sds(memory_state.shape, F32), small),
        in_specs=[VMEM] * 5,
        out_specs=[ANY] * 3,
        scratch_shapes=[
            pltpu.VMEM((rows, width), BF16),
            pltpu.VMEM((rows, heads), F32),
            pltpu.SemaphoreType.DMA,
            pltpu.SemaphoreType.DMA((2,)),
        ],
        compiler_params=pltpu.CompilerParams(vmem_limit_bytes=8 << 20),
        name="combine",
    )(new_memory, results, residual, picks, new_max)
    return layer_out, new_memory, new_max


def solution(mesh):
    both = ("grp", "ep")
    return jax.shard_map(
        body,
        mesh=mesh,
        in_specs=(
            P(both, None), P(both, None, None, None), P(both, None), P(),
            P(None, "ep"), P(None, "ep"), P(None, "ep"), P(None, "ep"),
            P(), P(), P(), P(), P(None, "ep"), P(),
            P(both, None), P(both, None),
            P("ep", None, None), P("ep", None, None), P("ep", None, None),
        ),
        out_specs=(P(both, None), P(both, None, None, None), P(both, None)),
        check_vma=False,
    )
```

```python
import functools

import jax
import jax.numpy as jnp
from jax import lax
from jax.experimental import pallas as pl
from jax.experimental.pallas import tpu as pltpu
from jax.sharding import PartitionSpec as P

epsilon = 1e-06
F32 = jnp.float32
BF16 = jnp.bfloat16
ANY = pl.BlockSpec(memory_space=pl.ANY)
HBM = pl.BlockSpec(memory_space=pltpu.HBM)
VMEM = pl.BlockSpec(memory_space=pltpu.VMEM)
SLOTS = 2


def scaled_norm(entries, gain):
    return entries * lax.rsqrt(jnp.mean(entries * entries, axis=-1, keepdims=True) + epsilon) * gain


def flip(me, mask):
    peer, bit = me, 1
    while bit <= mask:
        if mask & bit:
            peer = peer + bit * (1 - 2 * lax.rem(lax.div(me, bit), 2))
        bit *= 2
    return peer


def remote(source, target, send_sem, recv_sem, peer):
    return pltpu.make_async_remote_copy(
        src_ref=source, dst_ref=target, send_sem=send_sem, recv_sem=recv_sem, device_id={"ep": peer}
    )


def exchange(n, me, source, landing, send_sem, recv_sem):
    for mask in range(n - 1, 0, -1):
        peer = flip(me, mask)
        remote(source(peer), landing.at[me], send_sem, recv_sem(mask), peer).start()


def landed(blocks, sem):
    pltpu.make_async_copy(blocks, blocks, sem).wait()


def spread(n, me, source, target, send_sem, recv_sem):
    for mask in range(n - 2, 0, -2):
        remote(source(mask), target, send_sem, recv_sem(mask), flip(me, mask)).start()


def arrived(blocks, sem):
    remote(blocks, blocks, sem, sem, 0).wait_recv()


def departed(blocks, sem):
    remote(blocks, blocks, sem, sem, 0).wait_send()


def tall(table):
    return table if table.shape[1] % 128 == 0 else table.T


def across(lhs, table):
    return lax.dot_general(lhs, table, (((1,), (1,)), ((), ())), preferred_element_type=F32)


def apply(lhs, table):
    if table.shape[0] == lhs.shape[1]:
        return jnp.dot(lhs, table, preferred_element_type=F32)
    return across(lhs, table)


def rows_of(ref, n, start, size):
    return jnp.concatenate([ref[j, :, start : start + size].astype(F32) for j in range(n)], axis=0)


def layer_kernel(
    n, heads, key_size, value_size, names_width,
    tokens, memory, max_state, norm_gain, wv, wg, wq, wk, w_in, w_forget, forget_bias,
    head_gain, wo, expert_norm, routed, route_weights, w_gate, w_lift, w_down,
    new_memory, results, residual_out, picks_out, max_out,
    tok_s, max_s, ngain_s, vg_w, qk_w, gates_w, bias_s,
    hgain_s, o_w, egain_s, routed_s, rw_s, up_w, down_w,
    all_s, lhs_s, turned_w, names_s, pick_s, x_s, proj_s, back_s, kt_s, v_s, c_s, w_s, mix_s,
    res_s, needed_s, own_s, owned_s, out_s,
    local_sem, send_sem, column_sem, part_sem, group_sem,
):
    me = lax.axis_index("ep")
    barrier = pltpu.get_barrier_semaphore()
    for mask in range(n - 1, 0, -1):
        pl.semaphore_signal(barrier, inc=1, device_id={"ep": flip(me, mask)})
    rows, width = tokens.shape
    most, same = pl.ds(0, n - 1), pl.ds(0, n // 2 - 1)
    core, chip = lax.rem(me, 2), lax.div(me, 2)
    cq, cv = heads * key_size // n, heads * value_size // n
    columns = wo.shape[1] if wo.shape[0] == width else wo.shape[0]

    def part_of(table, size, start, count):
        at = pl.ds(pl.multiple_of(core * size, size) + start, count)
        return table.at[:, at] if table.shape[0] == width else table.at[at]

    shared = [
        part_of(vg_w, 2 * cv, 0, 2 * cv), part_of(qk_w, 2 * cq, 0, 2 * cq),
        part_of(o_w, columns, 0, columns),
    ]
    loads = [
        (tokens, tok_s, 0), (routed, routed_s, 1), (norm_gain, ngain_s, 2),
        (w_in, gates_w.at[0], 3), (w_forget, gates_w.at[1], 3), (forget_bias, bias_s, 4),
        (max_state, max_s, 5), (route_weights, rw_s, 6), (wv, part_of(vg_w, 2 * cv, 0, cv), 7),
        (wg, part_of(vg_w, 2 * cv, cv, cv), 7),
        (wq, part_of(qk_w, 2 * cq, 0, cq), 8),
        (wk, part_of(qk_w, 2 * cq, cq, cq), 8), (wo, shared[2], 10 + 1),
        *(
            (memory.at[s, h], new_memory.at[s, h], 9)
            for h in range(heads) for s in range(rows)
        ),
        (head_gain, hgain_s, 10), (expert_norm, egain_s, 12),
        (w_gate.at[0], up_w.at[0], 13), (w_lift.at[0], up_w.at[1], 13), (w_down.at[0], down_w, 14),
    ]
    for source, target, i in loads:
        pltpu.make_async_copy(source, target, local_sem.at[i]).start()

    for i, target in enumerate((tok_s, routed_s, ngain_s, gates_w, bias_s, max_s, rw_s)):
        landed(target, local_sem.at[i])
    lane = lax.broadcasted_iota(jnp.int32, (rows, names_width), 1)
    which = routed_s[...]
    weights = rw_s[...]
    taken = jnp.zeros((1, names_width), F32)
    chosen = []
    named = jnp.zeros((rows, names_width), F32)
    weighed = jnp.zeros((rows, names_width), F32)
    for slot in range(SLOTS):
        for k in range(which.shape[1]):
            hit = lane == which[:, k : k + 1] + slot * n
            named = named + hit.astype(F32)
            weighed = weighed + jnp.where(hit, weights[:, k : k + 1], 0.0)
    slot_of = (lax.broadcasted_iota(jnp.int32, (1, names_width), 1) >= n).astype(F32)
    for r in range(rows):
        chosen.append(named[r : r + 1] * (taken == slot_of).astype(F32))
        taken = taken + named[r : r + 1]
    chosen = jnp.concatenate(chosen, axis=0)
    for t in range(n // 2):
        proj_s[t, :, :names_width] = chosen.astype(BF16)
    picks_out[...] = chosen * weighed

    gain = ngain_s[...]
    own = scaled_norm(tok_s[...].astype(F32), gain).astype(BF16)
    input_logit = across(own, gates_w[0])
    raw = across(own, gates_w[1]) + bias_s[...]
    log_forget = jnp.minimum(raw, 0.0) - jnp.log1p(jnp.exp(-jnp.abs(raw)))
    prior = log_forget + max_s[...]
    new_max = jnp.maximum(prior, input_logit)
    max_out[...] = new_max
    carried = jnp.exp(prior - new_max)
    written = jnp.exp(input_logit - new_max) * key_size**-0.5

    pl.semaphore_wait(barrier, n - 1)
    spread(
        n, me, lambda mask: tok_s, all_s.at[chip], send_sem.at[0],
        lambda mask: group_sem.at[0 if mask < n // 2 else 7],
    )
    all_s[chip] = tok_s[...]
    partner = flip(me, 1)
    for i, block in enumerate(shared):
        landed(block, local_sem.at[(7, 8, 11)[i]])
        remote(block, block, send_sem.at[5 + heads + i], group_sem.at[3 + i], partner).start()
    per = n // heads
    arrived(shared[0], group_sem.at[3])
    arrived(shared[1], group_sem.at[4])
    turned_w[...] = qk_w[...].T

    def prepare(half):
        count = n // 4
        at = pl.ds(pl.multiple_of(half * count * rows, count * rows), count * rows)
        entries = [all_s[half * count + t].astype(F32) for t in range(count)]
        lhs_s[at, :] = scaled_norm(jnp.concatenate(entries, axis=0), gain).astype(BF16)

    half = lax.div(chip, n // 4)
    arrived(all_s.at[pl.ds(0, n // 4 - 1)], group_sem.at[0])
    prepare(half)
    arrived(all_s.at[pl.ds(0, n // 4)], group_sem.at[7])
    prepare(1 - half)
    gate_size = 2 * cv + 2 * cq
    for table, start, size in ((vg_w, names_width, 2 * cv), (turned_w, names_width + 2 * cv, 2 * cq)):
        made = apply(lhs_s[...], table[...]).astype(BF16).astype(F32)
        for t in range(n // 2):
            for c in range(2):
                proj_s[t, :, start + c * gate_size : start + c * gate_size + size] = (
                    made[t * rows : (t + 1) * rows, c * size : (c + 1) * size].astype(BF16)
                )
    spread(
        n, me, lambda mask: proj_s.at[flip(chip, mask // 2)], back_s.at[chip], send_sem.at[1],
        lambda mask: column_sem.at[mask // per],
    )
    back_s[chip] = proj_s[chip]

    at = pl.ds(pl.multiple_of(chip * 2 * columns, 2 * columns), 2 * columns)
    x_s[...] = jnp.concatenate([all_s[t, :, at].astype(F32) for t in range(n // 2)], axis=0)
    for i, target in ((10, hgain_s), (12, egain_s)):
        landed(target, local_sem.at[i])
    pltpu.make_async_copy(memory, new_memory, local_sem.at[9]).wait()
    for h in range(heads):
        c_s[h] = jnp.broadcast_to(carried[:, h : h + 1], (rows, value_size))
        w_s[h] = jnp.broadcast_to(written[:, h : h + 1], (rows, value_size))
    step = 32
    quarter = lax.div(me, per)
    pad = jnp.zeros((-rows % 8, 2 * key_size), F32)

    def read(h):
        pieces = [
            back_s[h * (per // 2) + t // 2][
                :, names_width + t % 2 * gate_size : names_width + (t % 2 + 1) * gate_size
            ].astype(F32)
            for t in range(per)
        ]
        v = jnp.concatenate([b[:, :cv] for b in pieces], axis=1)
        g = jnp.concatenate([b[:, cv : 2 * cv] for b in pieces], axis=1)
        qk = jnp.concatenate([b[:, 2 * cv :] for b in pieces], axis=1)
        turned = jnp.concatenate([qk, pad], axis=0).T
        query = jnp.concatenate([turned[t * 2 * cq : t * 2 * cq + cq] for t in range(per)], axis=0)
        key = jnp.concatenate([turned[t * 2 * cq + cq : (t + 1) * 2 * cq] for t in range(per)], axis=0)
        v = v * w_s[h]
        match = jnp.sum(query * key, axis=0, keepdims=True)
        gains = hgain_s[:, pl.ds(pl.multiple_of(h * value_size, value_size), value_size)]
        gains = gains * jax.nn.sigmoid(g)
        sums, own_match = [], []
        for s in range(rows):
            total = jnp.zeros((8, value_size), F32)
            for at in range(0, key_size, step):
                terms = query[at : at + step, s : s + 1] * new_memory[s, h, at : at + step, :]
                total = total + jnp.sum(terms.reshape(step // 8, 8, value_size), axis=0)
            sums.append(jnp.sum(total, axis=0, keepdims=True))
            own_match.append(match[:, s : s + 1] * v[s : s + 1])
        readout = c_s[h] * jnp.concatenate(sums, axis=0) + jnp.concatenate(own_match, axis=0)
        return scaled_norm(readout, gains).astype(BF16), key, v

    for i in range(heads):
        count = per // 2 if i else per // 2 - 1
        if count:
            arrived(back_s.at[pl.ds(0, count)], column_sem.at[i])
        h = flip(quarter, i)
        mix_s[h, chip], kt_s[h], v_s[h] = read(h)
        mine = mix_s.at[h, chip]
        spread(n, me, lambda mask: mine, mine, send_sem.at[2], lambda mask: group_sem.at[6])
    names_s[...] = jnp.concatenate(
        [back_s[t][:, :names_width].astype(F32) for t in range(n // 2)], axis=0
    ).T
    wanted = SLOTS * n // 2
    place = lax.broadcasted_iota(jnp.int32, (wanted, n // 2 * rows), 0)
    row = lax.broadcasted_iota(jnp.int32, (wanted, n // 2 * rows), 1)
    first = (place - place % SLOTS) // SLOTS * rows
    inside = (row >= first) & (row < first + rows)
    even = place % SLOTS == 0
    for j in range(n):
        value = jnp.where(even, names_s[j : j + 1, :], names_s[n + j : n + j + 1, :])
        pick_s[j] = jnp.where(inside, value, 0.0).astype(BF16)

    def update(h, carry):
        for s in range(rows):
            keep = c_s[h, s : s + 1, :]
            values = v_s[h, s : s + 1, :]

            def chunk(r, nothing):
                at = pl.ds(pl.multiple_of(r * step, step), step)
                new_memory[s, h, at, :] = (
                    keep * new_memory[s, h, at, :] + kt_s[h, at, s : s + 1] * values
                )
                return nothing

            lax.fori_loop(0, key_size // step, chunk, 0, unroll=True)
        return carry

    lax.fori_loop(0, heads, update, 0)
    arrived(mix_s.at[:, same], group_sem.at[6])
    arrived(shared[2], group_sem.at[5])
    mixed = jnp.concatenate(
        [
            jnp.concatenate([mix_s[h, t].astype(F32) for t in range(n // 2)], axis=0).astype(BF16)
            for h in range(heads)
        ],
        axis=1,
    )
    branch = apply(mixed, o_w[...]).astype(BF16)
    residual = (x_s[...] + branch.astype(F32)).astype(BF16)
    picked = jnp.dot(
        pick_s[...].reshape(n * wanted, n // 2 * rows), residual, preferred_element_type=F32
    ).astype(BF16)
    res_s[...] = picked
    exchange(
        n, me, lambda peer: res_s.at[pl.ds(pl.multiple_of(peer * wanted, wanted), wanted)],
        needed_s, send_sem.at[2 + heads], lambda mask: part_sem.at[mask // per],
    )
    needed_s[me] = res_s[pl.ds(pl.multiple_of(me * wanted, wanted), wanted)]
    whole = residual.astype(F32)
    for t in range(n // 2):
        own_s[t] = whole[t * rows : (t + 1) * rows].astype(BF16)
    owned_s[chip] = own_s[chip]
    landed(up_w, local_sem.at[13])
    landed(down_w, local_sem.at[14])
    span = per * columns
    gate_value = jnp.zeros((2 * wanted, up_w.shape[2]), F32)
    lift_value = jnp.zeros((2 * wanted, up_w.shape[2]), F32)
    square = jnp.zeros((2 * wanted, 1), F32)
    for i in range(heads):
        arrived(needed_s.at[pl.ds(0, per if i else per - 1)], part_sem.at[i])
        if i == heads - 2:
            spread(
                n, me, lambda mask: own_s.at[flip(chip, mask // 2)], owned_s.at[chip],
                send_sem.at[3 + heads], lambda mask: group_sem.at[1],
            )
        part = flip(quarter, i)
        block = jnp.concatenate(
            [
                jnp.concatenate(
                    [needed_s[part * per + t + c].astype(F32) for t in range(0, per, 2)], axis=1
                )
                for c in range(2)
            ],
            axis=0,
        )
        at = pl.ds(pl.multiple_of(part * span, span), span)
        square += jnp.sum(block * block, axis=1, keepdims=True)
        block = (block * egain_s[:, at]).astype(BF16)
        gate_value += jnp.dot(block, up_w[0, at, :], preferred_element_type=F32)
        lift_value += jnp.dot(block, up_w[1, at, :], preferred_element_type=F32)
    scale = lax.rsqrt(square / width + epsilon)
    gate_value, lift_value = gate_value * scale, lift_value * scale
    hidden = (jax.nn.silu(gate_value) * lift_value).astype(BF16)
    result = jnp.dot(hidden, down_w[...], preferred_element_type=F32)
    for j in range(n):
        at = j % 2 * wanted + j // 2 * SLOTS
        out_s[j] = result[at : at + SLOTS].astype(BF16)
    exchange(
        n, me, lambda peer: out_s.at[peer], results, send_sem.at[4 + heads],
        lambda mask: group_sem.at[2],
    )
    results[me] = out_s[me]
    arrived(owned_s.at[same], group_sem.at[1])
    residual_out[...] = jnp.concatenate([owned_s[t].astype(F32) for t in range(n // 2)], axis=1)
    departed(all_s.at[same], send_sem.at[0])
    departed(proj_s.at[same], send_sem.at[1])
    departed(mix_s.at[:, same], send_sem.at[2])
    for i, block in enumerate(shared):
        departed(block, send_sem.at[5 + heads + i])
    departed(needed_s.at[most], send_sem.at[2 + heads])
    departed(own_s.at[same], send_sem.at[3 + heads])
    arrived(out_s.at[most], group_sem.at[2])
    departed(out_s.at[most], send_sem.at[4 + heads])


def combine_kernel(
    memory, results, residual, picks, new_max_in,
    layer_out, new_memory, max_out,
    out_s, top_s, mem_sem, sem,
):
    n, slots, width = results.shape
    rows, heads = new_max_in.shape

    for h in range(heads):
        for s in range(rows):
            for at in range(0, memory.shape[2], memory.shape[2] // 4):
                block = (s, h, pl.ds(at, memory.shape[2] // 4))
                pltpu.make_async_copy(memory.at[block], new_memory.at[block], mem_sem).start()
    top_s[...] = new_max_in[...]
    top = pltpu.make_async_copy(top_s, max_out, sem.at[0])
    top.start()
    weights = picks[...]
    total = jnp.zeros((rows, width), F32)
    for j in range(n):
        block = results[j].astype(F32)
        for s in range(slots):
            weight = weights[:, s * n + j : s * n + j + 1]
            total = total + (weight * block[s : s + 1]).astype(BF16).astype(F32)
    out_s[...] = (residual[...] + total).astype(BF16)
    out = pltpu.make_async_copy(out_s, layer_out, sem.at[1])
    out.start()
    pltpu.make_async_copy(memory, new_memory, mem_sem).wait()
    top.wait()
    out.wait()


def body(
    tokens, memory_state, max_state, norm_gain, query_weight, key_weight, value_weight,
    output_gate, input_gate, forget_gate, forget_bias, head_gain, output_weight, expert_norm,
    routed_experts, route_weights, expert_gate, expert_lift, expert_down,
):
    n = lax.axis_size("ep")
    rows, width = tokens.shape
    _, heads, key_size, value_size = memory_state.shape
    hidden = expert_gate.shape[2]
    cq, cv, columns = query_weight.shape[1], value_weight.shape[1], output_weight.shape[1]
    wv, wg, wo = tall(value_weight), tall(output_gate), tall(output_weight)
    wq, wk = query_weight.T, key_weight.T
    vg_shape = (width, 4 * cv) if cv % 128 == 0 else (4 * cv, width)
    o_shape = (width, 2 * columns) if columns % 128 == 0 else (2 * columns, width)
    names_width = -(-SLOTS * n // 128) * 128
    total_cols = names_width + 4 * cq + 4 * cv
    wanted = SLOTS * n // 2
    sds = jax.ShapeDtypeStruct
    small = sds((rows, heads), F32)
    padded = -(-rows // 8) * 8
    new_memory, results, residual, picks, new_max = pl.pallas_call(
        functools.partial(layer_kernel, n, heads, key_size, value_size, names_width),
        out_shape=(
            pltpu.VMEM(memory_state.shape, F32),
            pltpu.VMEM((n, SLOTS, width), BF16),
            pltpu.VMEM((rows, width), F32),
            pltpu.VMEM((rows, names_width), F32),
            pltpu.VMEM((rows, heads), F32),
        ),
        in_specs=[HBM] * 19,
        out_specs=[VMEM] * 5,
        scratch_shapes=[
            pltpu.VMEM((rows, width), BF16),
            pltpu.VMEM((rows, heads), F32),
            pltpu.VMEM((1, width), F32),
            pltpu.VMEM(vg_shape, BF16),
            pltpu.VMEM((4 * cq, width), BF16),
            pltpu.VMEM((2, heads, width), BF16),
            pltpu.VMEM((1, heads), F32),
            pltpu.VMEM((1, width), F32),
            pltpu.VMEM(o_shape, BF16),
            pltpu.VMEM((1, width), F32),
            pltpu.VMEM(routed_experts.shape, jnp.int32),
            pltpu.VMEM(route_weights.shape, F32),
            pltpu.VMEM((2, width, hidden), BF16),
            pltpu.VMEM((hidden, width), BF16),
            pltpu.VMEM((n // 2, rows, width), BF16),
            pltpu.VMEM((n // 2 * rows, width), BF16),
            pltpu.VMEM((width, 4 * cq), BF16),
            pltpu.VMEM((names_width, n // 2 * rows), F32),
            pltpu.VMEM((n, wanted, n // 2 * rows), BF16),
            pltpu.VMEM((n // 2 * rows, 2 * columns), F32),
            pltpu.VMEM((n // 2, rows, total_cols), BF16),
            pltpu.VMEM((n // 2, rows, total_cols), BF16),
            pltpu.VMEM((heads, key_size, padded), F32),
            pltpu.VMEM((heads, rows, value_size), F32),
            pltpu.VMEM((heads, rows, value_size), F32),
            pltpu.VMEM((heads, rows, value_size), F32),
            pltpu.VMEM((heads, n // 2, rows, value_size), BF16),
            pltpu.VMEM((n * wanted, 2 * columns), BF16),
            pltpu.VMEM((n, wanted, 2 * columns), BF16),
            pltpu.VMEM((n // 2, rows, 2 * columns), BF16),
            pltpu.VMEM((n // 2, rows, 2 * columns), BF16),
            pltpu.VMEM((n, SLOTS, width), BF16),
            pltpu.SemaphoreType.DMA((15,)),
            pltpu.SemaphoreType.DMA((8 + heads,)),
            pltpu.SemaphoreType.DMA((heads,)),
            pltpu.SemaphoreType.DMA((heads,)),
            pltpu.SemaphoreType.DMA((8,)),
        ],
        compiler_params=pltpu.CompilerParams(
            collective_id=0, has_side_effects=True, vmem_limit_bytes=40 << 20
        ),
        name="layer",
    )(*(
        pltpu.with_memory_space_constraint(x, pltpu.HBM)
        for x in (
            tokens, memory_state, max_state, norm_gain.reshape(1, -1), wv, wg, wq, wk,
            input_gate.T, forget_gate.T, forget_bias.reshape(1, -1), head_gain.reshape(1, -1), wo,
            expert_norm.reshape(1, -1), routed_experts, route_weights,
            expert_gate, expert_lift, expert_down,
        )
    ))
    layer_out, new_memory, new_max = pl.pallas_call(
        combine_kernel,
        out_shape=(sds((rows, width), BF16), sds(memory_state.shape, F32), small),
        in_specs=[VMEM] * 5,
        out_specs=[ANY] * 3,
        scratch_shapes=[
            pltpu.VMEM((rows, width), BF16),
            pltpu.VMEM((rows, heads), F32),
            pltpu.SemaphoreType.DMA,
            pltpu.SemaphoreType.DMA((2,)),
        ],
        compiler_params=pltpu.CompilerParams(vmem_limit_bytes=8 << 20),
        name="combine",
    )(new_memory, results, residual, picks, new_max)
    return layer_out, new_memory, new_max


def solution(mesh):
    both = ("grp", "ep")
    return jax.shard_map(
        body,
        mesh=mesh,
        in_specs=(
            P(both, None), P(both, None, None, None), P(both, None), P(),
            P(None, "ep"), P(None, "ep"), P(None, "ep"), P(None, "ep"),
            P(), P(), P(), P(), P(None, "ep"), P(),
            P(both, None), P(both, None),
            P("ep", None, None), P("ep", None, None), P("ep", None, None),
        ),
        out_specs=(P(both, None), P(both, None, None, None), P(both, None)),
        check_vma=False,
    )
```
